256 devices in a mesh: sp: 16 (over y, x), tp: 16 (over z, core).
Axes of the slice: x: 4, y: 4, z: 8, core: 2. Of those that a mesh axis runs over, the one named last changes fastest.
Arguments:
- latent: bfloat16 [16384, 2048], P(('sp', 'tp')), may hold values from -1.5 to 1.5
- context: bfloat16 [512, 2048], P('sp'), may hold values from -6 to 6
- cond: bfloat16 [2048], replicated, may hold values from -6 to 6
- cond_context: bfloat16 [2048], replicated, may hold values from -6 to 6
- mod_weight: bfloat16 [3, 2048, 2048], P(None, 'sp', 'tp'), may hold values from -0.125 to 0.125
- norm_gain: bfloat16 [2048], replicated, may hold values from 0.099609375 to 1.8984375
- down_q: bfloat16 [2048, 768], P('tp'), may hold values from -0.125 to 0.125
- down_kv: bfloat16 [2048, 512], P('tp'), may hold values from -0.125 to 0.125
- rope_weight: bfloat16 [2048, 32], replicated, may hold values from -0.125 to 0.125
- qlat_gain: bfloat16 [768], replicated, may hold values from 0.099609375 to 1.8984375
- kvlat_gain: bfloat16 [512], replicated, may hold values from 0.099609375 to 1.8984375
- up_query: bfloat16 [768, 1536], P(None, 'tp'), may hold values from -0.21875 to 0.21875
- up_key: bfloat16 [512, 1024], P(None, 'tp'), may hold values from -0.25 to 0.25
- up_value: bfloat16 [512, 1024], P(None, 'tp'), may hold values from -0.25 to 0.25
- query_gain: float32 [96], replicated, may hold values from 0.5 to 8
- key_gain: float32 [96], replicated, may hold values from 0.5 to 8
- context_bias: float32 [16], P('tp'), may hold values from -2.2 to -0.7
- out_weight: bfloat16 [1024, 2048], P('tp'), may hold values from -48 to 48
Outputs:
- mixed: bfloat16 [16384, 2048], P(('sp', 'tp'))
The draws below stay inside these ranges and needn't reach their ends.
All inputs are finite; a program needn't handle non-finite values.
Results may differ from the reference program's by a relative error of at most 0.028.
The reference program's roundings to bfloat16 on the way count: a program that leaves them out, or rounds other values in their place, can miss the bound.
Values may be sent and summed in bfloat16 or wider, within the bound.
No kernel may reach another device: no remote copies, remote signals or barrier semaphores. Data moves between devices by JAX's collectives and lax.ppermute only.
A program may use at most 64 MiB of HBM per device.

```python
import math
import jax
import jax.numpy as jnp
from jax import lax

D = 2048
HEADS = 16
NOPE = 64
ROPE = 32
VDIM = 64
QRANK = 768
KVRANK = 512
GRID_W = 64
TOK_DEV = 1024
CTX_DEV = 32
TOKENS = 16384
CONTEXT = 512


def draw_gain_vector(key):
    return jax.random.uniform(key, (NOPE + ROPE,), jnp.float32, 1.1, 1.9)


def draw_query_gain(key, part):
    return draw_gain_vector(jax.random.fold_in(key, 11))


def draw_key_gain(key, part):
    return draw_gain_vector(jax.random.fold_in(key, 23))


def level_of(own_key, shape, cuts, smallest, largest):
    level = 1.0
    for position, blocks in cuts:
        heights = jax.random.uniform(jax.random.fold_in(jax.random.fold_in(own_key, 6), position), (blocks,), jnp.float32, smallest / len(cuts), largest / len(cuts))
        level = level * jnp.repeat(jnp.exp(heights), shape[position] // blocks).reshape((-1,) + (1,) * (len(shape) - 1 - position))
    return level


def bell_draw(own_key, shape, deviation, bound, cuts=(), held_as=jnp.bfloat16):
    level = level_of(own_key, shape, cuts, -0.22, 0.18) if cuts else 1.0
    result = jax.random.normal(own_key, shape, jnp.float32) * deviation * level
    return jnp.minimum(jnp.maximum(result, -bound), bound).astype(held_as)


def setup_inputs(seed: int = 0) -> dict:
    streams_of = jax.random.split(jax.random.key(seed), 19)
    latent = bell_draw(streams_of[0], (TOKENS, D), 0.25, 1.5, ((0, 256),))
    context = bell_draw(streams_of[1], (CONTEXT, D), 1.0, 6.0, ((0, 16),))
    cond = bell_draw(streams_of[2], (D,), 1.0, 6.0)
    cond_context = bell_draw(streams_of[3], (D,), 1.0, 6.0)
    mod_weight = bell_draw(streams_of[4], (3, D, D), D ** -0.5, 0.125, ((1, 16), (2, 16)))
    norm_gain = jnp.clip(1.0 + 0.18 * jax.random.normal(streams_of[5], (D,), jnp.float32), 0.099609375, 1.8984375).astype(jnp.bfloat16)
    down_q = bell_draw(streams_of[6], (D, QRANK), D ** -0.5, 0.125, ((0, 16),))
    down_kv = bell_draw(streams_of[7], (D, KVRANK), D ** -0.5, 0.125, ((0, 16),))
    rope_weight = bell_draw(streams_of[8], (D, ROPE), D ** -0.5, 0.125)
    qlat_gain = jnp.clip(1.0 + 0.18 * jax.random.normal(streams_of[9], (QRANK,), jnp.float32), 0.099609375, 1.8984375).astype(jnp.bfloat16)
    kvlat_gain = jnp.clip(1.0 + 0.18 * jax.random.normal(streams_of[10], (KVRANK,), jnp.float32), 0.099609375, 1.8984375).astype(jnp.bfloat16)
    up_query = bell_draw(streams_of[11], (QRANK, HEADS * (NOPE + ROPE)), QRANK ** -0.5, 0.21875, ((1, 16),))
    up_key = bell_draw(streams_of[12], (KVRANK, HEADS * NOPE), KVRANK ** -0.5, 0.25, ((1, 16),))
    up_value = bell_draw(streams_of[13], (KVRANK, HEADS * VDIM), KVRANK ** -0.5, 0.25, ((1, 16),))
    query_gain = draw_query_gain(jax.random.fold_in(streams_of[18], 71), 0)
    key_gain = draw_key_gain(jax.random.fold_in(streams_of[18], 71), 0)
    context_bias = jnp.clip(-2.2 + 1.5 * jax.random.uniform(streams_of[16], (HEADS,), jnp.float32) ** level_of(streams_of[16], (HEADS,), ((0, 16),), -0.2, 0.2), -2.2, -0.7)
    out_weight = bell_draw(streams_of[17], (HEADS * VDIM, D), (2.0 * (TOKENS + CONTEXT) ** 0.5 * (HEADS * VDIM) ** -0.5), 48.0, ((0, 16),))
    return dict(latent=latent, context=context, cond=cond, cond_context=cond_context, mod_weight=mod_weight, norm_gain=norm_gain, down_q=down_q, down_kv=down_kv, rope_weight=rope_weight, qlat_gain=qlat_gain, kvlat_gain=kvlat_gain, up_query=up_query, up_key=up_key, up_value=up_value, query_gain=query_gain, key_gain=key_gain, context_bias=context_bias, out_weight=out_weight)


epsilon = 1e-06
theta = 10000.0

def rounded(tensor):
    return lax.optimization_barrier(tensor.astype(jnp.bfloat16))

def rms_scale(tensor, gain):
    return tensor * lax.rsqrt(lax.optimization_barrier(jnp.mean(tensor * tensor, axis=-1, keepdims=True)) + epsilon) * gain.astype(jnp.float32)

def axial_tables(positions):
    pair_count = ROPE // 4
    frequency = jnp.power(theta, -jnp.arange(pair_count, dtype=jnp.float32) / pair_count)
    row_angle = (positions // GRID_W).astype(jnp.float32)[:, None] * frequency
    col_angle = (positions % GRID_W).astype(jnp.float32)[:, None] * frequency
    return (jnp.cos(row_angle), jnp.sin(row_angle), jnp.cos(col_angle), jnp.sin(col_angle))

def rotate_half(tensor, cosine, sine_table):
    first, second = jnp.split(tensor, 2, axis=-1)
    cosine = cosine[:, None, :]
    sine_table = sine_table[:, None, :]
    return jnp.concatenate([first * cosine - second * sine_table, second * cosine + first * sine_table], axis=-1)

def axial_rotate(tensor, tables):
    half_width = tensor.shape[-1] // 2
    return jnp.concatenate([rotate_half(tensor[..., :half_width], tables[0], tables[1]), rotate_half(tensor[..., half_width:], tables[2], tables[3])], axis=-1)

def modulate(row_block, gain, shifts, scales):
    normal = rms_scale(row_block.astype(jnp.float32), gain)
    return rounded(normal * (1.0 + scales) + shifts)

def make_queries(query_latent, up_query, query_gain, tables):
    amount = query_latent.shape[0]
    projected = jnp.dot(query_latent, up_query, preferred_element_type=jnp.float32).reshape(amount, -1, NOPE + ROPE)
    normal = rms_scale(projected, query_gain)
    return rounded(jnp.concatenate([normal[..., :NOPE], axial_rotate(normal[..., NOPE:], tables)], axis=-1))

def make_keys(kv_latent, rope_rows, up_key, up_value, key_gain, tables):
    amount = kv_latent.shape[0]
    unrotated = jnp.dot(kv_latent, up_key, preferred_element_type=jnp.float32).reshape(amount, -1, NOPE)
    head_count = unrotated.shape[1]
    shared = jnp.broadcast_to(rope_rows.astype(jnp.float32)[:, None, :], (amount, head_count, ROPE))
    normal = rms_scale(jnp.concatenate([unrotated, shared], axis=-1), key_gain)
    if tables is not None:
        normal = jnp.concatenate([normal[..., :NOPE], axial_rotate(normal[..., NOPE:], tables)], axis=-1)
    values = jnp.dot(kv_latent, up_value, preferred_element_type=jnp.float32).reshape(amount, head_count, VDIM)
    return (rounded(normal), rounded(values))

def attend(query_block, keys, values, context_keys, context_values, context_shift):
    scaling = (NOPE + ROPE) ** (-0.5)
    query_wide = query_block.astype(jnp.float32)
    latent_scores = jnp.einsum('qhd,khd->qhk', query_wide, keys.astype(jnp.float32)) * scaling
    context_scores = jnp.einsum('qhd,khd->qhk', query_wide, context_keys.astype(jnp.float32)) * scaling
    context_scores = context_scores + context_shift[None, :, None]
    row_max = jnp.maximum(lax.optimization_barrier(jnp.max(latent_scores, axis=-1)), lax.optimization_barrier(jnp.max(context_scores, axis=-1)))[..., None]
    latent_weights = jnp.exp(latent_scores - row_max)
    context_weights = jnp.exp(context_scores - row_max)
    totals = lax.optimization_barrier(jnp.sum(latent_weights, axis=-1)) + lax.optimization_barrier(jnp.sum(context_weights, axis=-1))
    summed = jnp.einsum('qhk,khd->qhd', rounded(latent_weights).astype(jnp.float32), values.astype(jnp.float32))
    summed = summed + jnp.einsum('qhk,khd->qhd', rounded(context_weights).astype(jnp.float32), context_values.astype(jnp.float32))
    return rounded(summed / totals[..., None])

def reference(latent, context, cond, cond_context, mod_weight, norm_gain, down_q, down_kv, rope_weight, qlat_gain, kvlat_gain, up_query, up_key, up_value, query_gain, key_gain, context_bias, out_weight):
    activated = rounded(jax.nn.silu(jnp.stack([cond, cond_context]).astype(jnp.float32)))
    shifts, scales, gates = (jnp.dot(activated[0], mod_weight[member], preferred_element_type=jnp.float32) for member in range(3))
    context_shift, context_scale = (jnp.dot(activated[1], mod_weight[member], preferred_element_type=jnp.float32) for member in range(2))
    normed = modulate(latent, norm_gain, shifts, scales)
    context_normed = modulate(context, norm_gain, context_shift, context_scale)
    query_latent = rounded(rms_scale(jnp.dot(normed, down_q, preferred_element_type=jnp.float32), qlat_gain))
    kv_latent = rounded(rms_scale(jnp.dot(normed, down_kv, preferred_element_type=jnp.float32), kvlat_gain))
    context_kv = rounded(rms_scale(jnp.dot(context_normed, down_kv, preferred_element_type=jnp.float32), kvlat_gain))
    rope_rows = rounded(jnp.dot(normed, rope_weight, preferred_element_type=jnp.float32))
    context_rope = rounded(jnp.dot(context_normed, rope_weight, preferred_element_type=jnp.float32))
    tables = axial_tables(jnp.arange(TOKENS, dtype=jnp.int32))
    queries = make_queries(query_latent, up_query, query_gain, tables)
    keys, values = make_keys(kv_latent, rope_rows, up_key, up_value, key_gain, tables)
    context_keys, context_values = make_keys(context_kv, context_rope, up_key, up_value, key_gain, None)
    context_shift_heads = context_bias.astype(jnp.float32) + math.log(TOK_DEV / CTX_DEV)
    block_rows = math.gcd(TOKENS, 256)
    query_blocks = queries.reshape(TOKENS // block_rows, block_rows, HEADS, NOPE + ROPE)
    attended = lax.map(lambda blocks: attend(blocks, keys, values, context_keys, context_values, context_shift_heads), query_blocks)
    attended = attended.reshape(TOKENS, HEADS * VDIM)
    projected = jnp.dot(attended, out_weight, preferred_element_type=jnp.float32)
    return (latent.astype(jnp.float32) + gates * projected).astype(jnp.bfloat16)
```

```python
import functools
import math

import jax
import jax.numpy as jnp
from jax import lax
from jax.experimental import pallas as pl
from jax.experimental.pallas import tpu as pltpu
from jax.sharding import Mesh
from jax.sharding import PartitionSpec as P

NOPE = 64
ROPE = 32
HEAD = NOPE + ROPE
VDIM = 64
GRID_W = 64
TOK_DEV = 1024
CTX_DEV = 32
QRANK = 768
KVRANK = 512
KV_PAD = 640
CTX_PAD = 128
SP = ("y", "x")
SP_TP = ("y", "x", "tp")
BF16 = jnp.bfloat16
F32 = jnp.float32


epsilon = 1e-06
theta = 10000.0
SCALE = HEAD**-0.5 * math.log2(math.e)


def rms_scale(tensor, gain):
    return (
        tensor
        * lax.rsqrt(jnp.mean(tensor * tensor, axis=-1, keepdims=True) + epsilon)
        * gain.astype(F32)
    )


def modulate(row_block, gain, shifts, scales):
    normal = rms_scale(row_block.astype(F32), gain)
    return (normal * (1.0 + scales) + shifts).astype(BF16)


def gathered(block, axis):
    count = lax.axis_size(axis)
    sent = jnp.broadcast_to(block[None], (count,) + block.shape)
    return lax.all_to_all(sent, axis, 0, 0, tiled=True)


def shifted(block, axis, step):
    count = lax.axis_size(axis)
    return lax.ppermute(block, axis, [(i, (i + step) % count) for i in range(count)])


def rope_tables(positions):
    pair_count = ROPE // 4
    frequency = jnp.power(theta, -jnp.arange(pair_count, dtype=F32) / pair_count)[:, None]
    row_angle = (positions // GRID_W).astype(F32)[None, :] * frequency
    col_angle = (positions % GRID_W).astype(F32)[None, :] * frequency
    return jnp.concatenate(
        [jnp.cos(row_angle), jnp.sin(row_angle), jnp.cos(col_angle), jnp.sin(col_angle)], axis=0
    )


def nt(a, b):
    return lax.dot_general(a, b, (((1,), (1,)), ((), ())), preferred_element_type=F32)


def tn(a, b):
    return lax.dot_general(a, b, (((0,), (0,)), ((), ())), preferred_element_type=F32)


def head_norm(u, gain):
    scale = lax.rsqrt(jnp.sum(u * u, axis=0, keepdims=True) * (1.0 / HEAD) + epsilon)
    return u * scale * gain


def rotated(n, tables):
    a, b, c, d = (n[NOPE + 8 * i : NOPE + 8 * i + 8] for i in range(4))
    cos_r, sin_r, cos_c, sin_c = (tables[8 * i : 8 * i + 8] for i in range(4))
    return jnp.concatenate(
        [
            n[:NOPE],
            a * cos_r - b * sin_r,
            b * cos_r + a * sin_r,
            c * cos_c - d * sin_c,
            d * cos_c + c * sin_c,
        ],
        axis=0,
    )


def query_body(lat_ref, up_ref, gain_ref, tab_ref, out_ref):
    u = nt(up_ref[...], lat_ref[:, :QRANK])
    out_ref[...] = rotated(head_norm(u, gain_ref[...]), tab_ref[...]).astype(BF16)


def key_body(lat_ref, ctx_ref, up_ref, gain_ref, tab_ref, out_ref):
    up = up_ref[...]
    gain = gain_ref[...]
    u = nt(up, lat_ref[:, QRANK:])
    tokens = u.shape[1]
    out_ref[:HEAD, :tokens] = rotated(head_norm(u[:HEAD], gain), tab_ref[...]).astype(BF16)
    out_ref[HEAD:, :tokens] = u[HEAD:].astype(BF16)
    w = nt(up, ctx_ref[...])
    out_ref[:HEAD, tokens:] = head_norm(w[:HEAD], gain).astype(BF16)
    out_ref[HEAD:, tokens:] = w[HEAD:].astype(BF16)


def attend_body(bias_ref, q_ref, *refs, block):
    kv_refs, out_ref = refs[:-1], refs[-1]
    tokens = q_ref.shape[1]
    ctx = functools.reduce(lambda s, r: s + r[:, tokens:].astype(F32), kv_refs, 0.0).astype(BF16)
    ones = jnp.ones((16, tokens), BF16)
    parts = [(r[:HEAD, :tokens], r[HEAD:, :tokens], None) for r in kv_refs]
    parts.append((ctx[:HEAD], ctx[HEAD:], bias_ref[0]))

    @pl.loop(0, tokens // block)
    def _(i):
        at = pl.ds(pl.multiple_of(i * block, block), block)
        q = q_ref[:, at]
        scores = []
        for key, _, bias in parts:
            s = tn(key, q) * SCALE
            scores.append(s if bias is None else s + bias)
        top = functools.reduce(
            jnp.maximum, [jnp.max(s, axis=0, keepdims=True) for s in scores]
        )
        acc = 0.0
        for s, (_, value, _) in zip(scores, parts):
            weights = jnp.exp2(s - top).astype(BF16)
            with_ones = jnp.concatenate([value, ones[:, : value.shape[1]]], axis=0)
            acc = acc + jnp.dot(with_ones, weights, preferred_element_type=F32)
        total = acc[VDIM : VDIM + 1]
        out_ref[:VDIM, at] = (acc[:VDIM] / total).astype(BF16)
        lse = top + jnp.log2(total)
        hi = lse.astype(BF16).astype(F32)
        mid = (lse - hi).astype(BF16).astype(F32)
        low = lse - hi - mid
        zeros = jnp.zeros((13, block), F32)
        out_ref[VDIM:, at] = jnp.concatenate([hi, mid, low, zeros], axis=0).astype(BF16)


def merge_body(*refs):
    parts, out_ref = refs[:-1], refs[-1]
    lses, outs = [], []
    for r in parts:
        tail = r[VDIM:, :].astype(F32)
        lses.append(tail[0:1] + tail[1:2] + tail[2:3])
        outs.append(r[:VDIM, :].astype(F32))
    top = functools.reduce(jnp.maximum, lses)
    weights = [jnp.exp2(s - top) for s in lses]
    total = functools.reduce(jnp.add, weights)
    acc = functools.reduce(jnp.add, [w * o for w, o in zip(weights, outs)])
    out_ref[...] = (acc / total).T.astype(BF16)


def kernel(body, shape, scalars, arrays, flops=0):
    vmem = pl.BlockSpec(memory_space=pltpu.VMEM)
    smem = pl.BlockSpec(memory_space=pltpu.SMEM)
    return pl.pallas_call(
        body,
        out_shape=jax.ShapeDtypeStruct(shape, BF16),
        in_specs=[smem] * len(scalars) + [vmem] * len(arrays),
        out_specs=vmem,
        cost_estimate=pl.CostEstimate(flops=flops, bytes_accessed=0, transcendentals=0),
        compiler_params=pltpu.CompilerParams(vmem_limit_bytes=28 << 20),
    )(*scalars, *arrays)


def shards(
    latent,
    context,
    cond,
    cond_context,
    mod_weight,
    norm_gain,
    down_q,
    down_kv,
    rope_weight,
    qlat_gain,
    kvlat_gain,
    up_query,
    up_key,
    up_value,
    query_gain,
    key_gain,
    context_bias,
    out_weight,
):
    seq_index = lax.axis_index(SP)
    tp_count = lax.axis_size("tp")
    own_rows = latent.shape[0]
    block_tokens = own_rows * tp_count
    row_span = mod_weight.shape[1]
    down = lax.all_gather(
        jnp.concatenate([down_q, down_kv], axis=1), "tp", axis=0, tiled=True
    )
    out_rows = lax.all_gather(out_weight, "tp", axis=0, tiled=True)

    activated = jax.nn.silu(jnp.stack([cond, cond_context]).astype(F32)).astype(BF16)
    own_part = lax.dynamic_slice_in_dim(activated, seq_index * row_span, row_span, 1)
    partial_value = jnp.concatenate(
        [
            jnp.einsum("d,rde->re", own_part[0], mod_weight, preferred_element_type=F32),
            jnp.einsum("d,rde->re", own_part[1], mod_weight[:2], preferred_element_type=F32),
            jnp.zeros((3, mod_weight.shape[2]), F32),
        ],
        axis=0,
    )
    summed = jnp.sum(gathered(partial_value, SP).reshape((-1,) + partial_value.shape), axis=0)
    modulations = jnp.swapaxes(gathered(summed, "tp").reshape((-1,) + summed.shape), 0, 1)
    modulations = modulations.reshape(summed.shape[0], -1)

    positions = seq_index * block_tokens + jnp.arange(block_tokens, dtype=jnp.int32)
    tables = rope_tables(positions)
    up_kv = jnp.concatenate(
        [
            jnp.pad(up_key.T, ((0, 0), (0, KV_PAD - KVRANK))),
            jnp.eye(ROPE, KV_PAD, KVRANK, dtype=BF16),
            jnp.pad(up_value.T, ((0, 0), (0, KV_PAD - KVRANK))),
        ],
        axis=0,
    )

    normed = modulate(latent, norm_gain, modulations[0], modulations[1])
    context_normed = modulate(context, norm_gain, modulations[3], modulations[4])
    stacked = jnp.concatenate([normed, context_normed], axis=0)
    query_down = jnp.dot(normed, down[:, :QRANK], preferred_element_type=F32)
    kv_down = jnp.dot(stacked, down[:, QRANK:], preferred_element_type=F32)
    query_latent = rms_scale(query_down, qlat_gain).astype(BF16)
    kv_latent = rms_scale(kv_down, kvlat_gain).astype(BF16)
    rope_rows = jnp.dot(stacked, rope_weight, preferred_element_type=F32).astype(BF16)
    room = jnp.zeros((stacked.shape[0], KV_PAD - KVRANK - ROPE), BF16)
    kv_rows = jnp.concatenate([kv_latent, rope_rows, room], axis=1)
    latents = lax.all_gather(
        jnp.concatenate([query_latent, kv_rows[:own_rows]], axis=1), "tp", axis=0, tiled=True
    )
    place = jnp.arange(CTX_PAD, dtype=jnp.int32)[:, None] // CTX_DEV == lax.axis_index("y")
    context_rows = jnp.where(place, jnp.tile(kv_rows[own_rows:], (CTX_PAD // CTX_DEV, 1)), 0)
    context_rows = context_rows.astype(BF16)

    kv = kernel(
        key_body,
        (HEAD + VDIM, block_tokens + CTX_PAD),
        (),
        (latents, context_rows, up_kv, key_gain[:, None], tables),
    )
    kvs = [kv] + [shifted(kv, "y", k) for k in range(1, 4)]
    q = kernel(
        query_body, (HEAD, block_tokens), (), (latents, up_query.T, query_gain[:, None], tables)
    )
    qs = [shifted(q, "x", k) for k in range(1, 4)] + [q]
    bias = (context_bias + math.log(TOK_DEV / CTX_DEV)) * math.log2(math.e)
    attend = functools.partial(attend_body, block=512)
    partials = [
        kernel(attend, (VDIM + 16, block_tokens), (bias,), (block, *kvs), flops=3_000_000_000)
        for block in qs
    ]
    back = [shifted(part, "x", -k) for k, part in zip(range(1, 4), partials[:3])]
    attended = kernel(merge_body, (block_tokens, VDIM), (), (partials[3], *back))

    token_rows = lax.all_to_all(attended, "tp", split_axis=0, concat_axis=1, tiled=True)
    projected = jnp.dot(token_rows, out_rows, preferred_element_type=F32)
    return (latent.astype(F32) + modulations[2] * projected).astype(BF16)


def solution(mesh):
    split = Mesh(mesh.devices.reshape(4, 4, mesh.shape["tp"]), ("y", "x", "tp"))
    placed = (
        P(SP_TP, None),
        P(SP, None),
        P(),
        P(),
        P(None, SP, "tp"),
        P(),
        P("tp", None),
        P("tp", None),
        P(),
        P(),
        P(),
        P(None, "tp"),
        P(None, "tp"),
        P(None, "tp"),
        P(),
        P(),
        P("tp"),
        P("tp", None),
    )
    return jax.shard_map(
        shards, mesh=split, in_specs=placed, out_specs=P(SP_TP, None), check_vma=False
    )
```

```python
import functools
import math

import jax
import jax.numpy as jnp
from jax import lax
from jax.experimental import pallas as pl
from jax.experimental.pallas import tpu as pltpu
from jax.sharding import Mesh
from jax.sharding import PartitionSpec as P

NOPE = 64
ROPE = 32
HEAD = NOPE + ROPE
VDIM = 64
GRID_W = 64
TOK_DEV = 1024
CTX_DEV = 32
QRANK = 768
KVRANK = 512
KV_PAD = 640
CTX_PAD = 128
SP = ("y", "x")
SP_TP = ("y", "x", "tp")
BF16 = jnp.bfloat16
F32 = jnp.float32


epsilon = 1e-06
theta = 10000.0
SCALE = HEAD**-0.5 * math.log2(math.e)


def rms_scale(tensor, gain):
    return (
        tensor
        * lax.rsqrt(jnp.mean(tensor * tensor, axis=-1, keepdims=True) + epsilon)
        * gain.astype(F32)
    )


def modulate(row_block, gain, shifts, scales):
    normal = rms_scale(row_block.astype(F32), gain)
    return (normal * (1.0 + scales) + shifts).astype(BF16)


def gathered(block, axis):
    count = lax.axis_size(axis)
    sent = jnp.broadcast_to(block[None], (count,) + block.shape)
    return lax.all_to_all(sent, axis, 0, 0, tiled=True)


def shifted(block, axis, step):
    count = lax.axis_size(axis)
    return lax.ppermute(block, axis, [(i, (i + step) % count) for i in range(count)])


def rope_tables(positions):
    pair_count = ROPE // 4
    frequency = jnp.power(theta, -jnp.arange(pair_count, dtype=F32) / pair_count)[:, None]
    row_angle = (positions // GRID_W).astype(F32)[None, :] * frequency
    col_angle = (positions % GRID_W).astype(F32)[None, :] * frequency
    return jnp.concatenate(
        [jnp.cos(row_angle), jnp.sin(row_angle), jnp.cos(col_angle), jnp.sin(col_angle)], axis=0
    )


def nt(a, b):
    return lax.dot_general(a, b, (((1,), (1,)), ((), ())), preferred_element_type=F32)


def tn(a, b):
    return lax.dot_general(a, b, (((0,), (0,)), ((), ())), preferred_element_type=F32)


def head_norm(u, gain):
    scale = lax.rsqrt(jnp.sum(u * u, axis=0, keepdims=True) * (1.0 / HEAD) + epsilon)
    return u * scale * gain


def rotated(n, tables):
    a, b, c, d = (n[NOPE + 8 * i : NOPE + 8 * i + 8] for i in range(4))
    cos_r, sin_r, cos_c, sin_c = (tables[8 * i : 8 * i + 8] for i in range(4))
    return jnp.concatenate(
        [
            n[:NOPE],
            a * cos_r - b * sin_r,
            b * cos_r + a * sin_r,
            c * cos_c - d * sin_c,
            d * cos_c + c * sin_c,
        ],
        axis=0,
    )


def make_body(
    lat_hbm, upq_hbm, upkv_hbm, ctx_ref, qgain_ref, kgain_ref, tab_ref, kv_ref, q_ref, *scratch
):
    kv_lat, q_lat, upkv, upq, sems = scratch
    tokens = q_lat.shape[0]
    copies = [
        pltpu.make_async_copy(upkv_hbm, upkv, sems.at[0]),
        pltpu.make_async_copy(lat_hbm.at[:, QRANK:], kv_lat, sems.at[1]),
        pltpu.make_async_copy(upq_hbm, upq, sems.at[2]),
        pltpu.make_async_copy(lat_hbm.at[:, :QRANK], q_lat, sems.at[3]),
    ]
    for copy in copies:
        copy.start()
    gain = kgain_ref[...]
    copies[0].wait()
    w = nt(upkv[...], ctx_ref[...])
    kv_ref[:HEAD, tokens:] = head_norm(w[:HEAD], gain).astype(BF16)
    kv_ref[HEAD:, tokens:] = w[HEAD:].astype(BF16)
    copies[1].wait()
    u = nt(upkv[...], kv_lat[...])
    kv_ref[:HEAD, :tokens] = rotated(head_norm(u[:HEAD], gain), tab_ref[...]).astype(BF16)
    kv_ref[HEAD:, :tokens] = u[HEAD:].astype(BF16)
    copies[2].wait()
    copies[3].wait()
    t = nt(upq[...], q_lat[...])
    q_ref[...] = rotated(head_norm(t, qgain_ref[...]), tab_ref[...]).astype(BF16)


def attend_body(bias_ref, q_ref, *refs, chunks, span, ahead, block):
    kv_refs, out_ref = refs[:-1], refs[-1]
    tokens = q_ref.shape[1]
    ones = jnp.ones((16, span), BF16)
    spans = [(r, a) for r in kv_refs[:chunks] for a in range(0, tokens, span)]
    if len(kv_refs) == 4:
        ctx = functools.reduce(lambda s, r: s + r[:, tokens:].astype(F32), kv_refs, 0.0)
        ctx = ctx.astype(BF16)
        spans.append((None, 0))

    @pl.loop(0, tokens // block)
    def _(i):
        at = pl.ds(pl.multiple_of(i * block, block), block)
        q = q_ref[:, at]

        def scores(j):
            ref, a = spans[j]
            key = ctx[:HEAD] if ref is None else ref[:HEAD, a : a + span]
            s = tn(key, q) * SCALE
            return s + bias_ref[0] if ref is None else s

        def summands(j):
            ref, a = spans[j]
            value = ctx[HEAD:] if ref is None else ref[HEAD:, a : a + span]
            return jnp.concatenate([value, ones[:, : value.shape[1]]], axis=0)

        top = acc = None
        coming = [scores(j) for j in range(min(ahead, len(spans)))]
        for j in range(len(spans)):
            s = coming.pop(0)
            here = jnp.max(s, axis=0, keepdims=True)
            if j + ahead < len(spans):
                coming.append(scores(j + ahead))
            new_top = here if top is None else jnp.maximum(top, here)
            weights = jnp.exp2(s - new_top).astype(BF16)
            add = jnp.dot(summands(j), weights, preferred_element_type=F32)
            acc = add if acc is None else acc * jnp.exp2(top - new_top) + add
            top = new_top
        total = acc[VDIM : VDIM + 1]
        out_ref[:VDIM, at] = (acc[:VDIM] / total).astype(BF16)
        lse = top + jnp.log2(total)
        hi = lse.astype(BF16).astype(F32)
        mid = (lse - hi).astype(BF16).astype(F32)
        low = lse - hi - mid
        zeros = jnp.zeros((13, block), F32)
        out_ref[VDIM:, at] = jnp.concatenate([hi, mid, low, zeros], axis=0).astype(BF16)


def merge_body(*refs):
    parts, out_ref = refs[:-1], refs[-1]
    lses, outs = [], []
    for r in parts:
        tail = r[VDIM:, :].astype(F32)
        lses.append(tail[0:1] + tail[1:2] + tail[2:3])
        outs.append(r[:VDIM, :].astype(F32))
    top = functools.reduce(jnp.maximum, lses)
    weights = [jnp.exp2(s - top) for s in lses]
    total = functools.reduce(jnp.add, weights)
    acc = functools.reduce(jnp.add, [w * o for w, o in zip(weights, outs)])
    out_ref[...] = (acc / total).T.astype(BF16)


def kernel(body, shape, scalars, arrays, flops=0, after=()):
    count = len(scalars) + len(arrays)
    ordered = tuple(after)

    def with_order(*refs):
        body(*refs[:count], refs[-1])

    vmem = pl.BlockSpec(memory_space=pltpu.VMEM)
    smem = pl.BlockSpec(memory_space=pltpu.SMEM)
    return pl.pallas_call(
        with_order,
        out_shape=jax.ShapeDtypeStruct(shape, BF16),
        in_specs=[smem] * len(scalars)
        + [vmem] * len(arrays)
        + [pl.BlockSpec(memory_space=pl.ANY)] * len(ordered),
        out_specs=vmem,
        cost_estimate=pl.CostEstimate(flops=flops, bytes_accessed=0, transcendentals=0),
        compiler_params=pltpu.CompilerParams(vmem_limit_bytes=28 << 20),
    )(*scalars, *arrays, *ordered)


def make_heads(latents, up_query, up_kv, context_rows, query_gain, key_gain, tables):
    vmem = pl.BlockSpec(memory_space=pltpu.VMEM)
    hbm = pl.BlockSpec(memory_space=pltpu.HBM)
    tokens = latents.shape[0]
    return pl.pallas_call(
        make_body,
        out_shape=(
            jax.ShapeDtypeStruct((HEAD + VDIM, tokens + CTX_PAD), BF16),
            jax.ShapeDtypeStruct((HEAD, tokens), BF16),
        ),
        in_specs=[hbm] * 3 + [vmem] * 4,
        out_specs=(vmem, vmem),
        scratch_shapes=[
            pltpu.VMEM((tokens, KV_PAD), BF16),
            pltpu.VMEM((tokens, QRANK), BF16),
            pltpu.VMEM(up_kv.shape, BF16),
            pltpu.VMEM(up_query.shape, BF16),
            pltpu.SemaphoreType.DMA((4,)),
        ],
        cost_estimate=pl.CostEstimate(flops=500_000_000, bytes_accessed=0, transcendentals=0),
        compiler_params=pltpu.CompilerParams(vmem_limit_bytes=58 << 20),
    )(latents, up_query, up_kv, context_rows, query_gain[:, None], key_gain[:, None], tables)


def shards(
    latent,
    context,
    cond,
    cond_context,
    mod_weight,
    norm_gain,
    down_q,
    down_kv,
    rope_weight,
    qlat_gain,
    kvlat_gain,
    up_query,
    up_key,
    up_value,
    query_gain,
    key_gain,
    context_bias,
    out_weight,
):
    seq_index = lax.axis_index(SP)
    tp_count = lax.axis_size("tp")
    own_rows = latent.shape[0]
    block_tokens = own_rows * tp_count
    row_span = mod_weight.shape[1]
    down = lax.all_gather(
        jnp.concatenate([down_q, down_kv], axis=1), "tp", axis=0, tiled=True
    )
    out_rows = lax.all_gather(out_weight, "tp", axis=0, tiled=True)

    activated = jax.nn.silu(jnp.stack([cond, cond_context]).astype(F32)).astype(BF16)
    own_part = lax.dynamic_slice_in_dim(activated, seq_index * row_span, row_span, 1)
    partial_value = jnp.concatenate(
        [
            jnp.einsum("d,rde->re", own_part[0], mod_weight, preferred_element_type=F32),
            jnp.einsum("d,rde->re", own_part[1], mod_weight[:2], preferred_element_type=F32),
            jnp.zeros((3, mod_weight.shape[2]), F32),
        ],
        axis=0,
    )
    summed = jnp.sum(gathered(partial_value, SP).reshape((-1,) + partial_value.shape), axis=0)
    modulations = jnp.swapaxes(gathered(summed, "tp").reshape((-1,) + summed.shape), 0, 1)
    modulations = modulations.reshape(summed.shape[0], -1)

    positions = seq_index * block_tokens + jnp.arange(block_tokens, dtype=jnp.int32)
    tables = rope_tables(positions)
    up_kv = jnp.concatenate(
        [
            jnp.pad(up_key.T, ((0, 0), (0, KV_PAD - KVRANK))),
            jnp.eye(ROPE, KV_PAD, KVRANK, dtype=BF16),
            jnp.pad(up_value.T, ((0, 0), (0, KV_PAD - KVRANK))),
        ],
        axis=0,
    )

    normed = modulate(latent, norm_gain, modulations[0], modulations[1])
    context_normed = modulate(context, norm_gain, modulations[3], modulations[4])
    stacked = jnp.concatenate([normed, context_normed], axis=0)
    query_down = jnp.dot(normed, down[:, :QRANK], preferred_element_type=F32)
    kv_down = jnp.dot(stacked, down[:, QRANK:], preferred_element_type=F32)
    query_latent = rms_scale(query_down, qlat_gain).astype(BF16)
    kv_latent = rms_scale(kv_down, kvlat_gain).astype(BF16)
    rope_rows = jnp.dot(stacked, rope_weight, preferred_element_type=F32).astype(BF16)
    room = jnp.zeros((stacked.shape[0], KV_PAD - KVRANK - ROPE), BF16)
    kv_rows = jnp.concatenate([kv_latent, rope_rows, room], axis=1)
    latents = lax.all_gather(
        jnp.concatenate([query_latent, kv_rows[:own_rows]], axis=1), "tp", axis=0, tiled=True
    )
    place = jnp.arange(CTX_PAD, dtype=jnp.int32)[:, None] // CTX_DEV == lax.axis_index("y")
    context_rows = jnp.where(place, jnp.tile(kv_rows[own_rows:], (CTX_PAD // CTX_DEV, 1)), 0)
    context_rows = context_rows.astype(BF16)

    kv, q = make_heads(latents, up_query.T, up_kv, context_rows, query_gain, key_gain, tables)
    kvs = [kv] + [shifted(kv, "y", k) for k in range(1, 4)]
    qs = [shifted(q, "x", k) for k in range(1, 4)]
    bias = (context_bias + math.log(TOK_DEV / CTX_DEV)) * math.log2(math.e)

    def attend(block, chunks, *arrays, after=()):
        body = functools.partial(attend_body, chunks=chunks, span=256, ahead=2, block=512)
        shape = (VDIM + 16, block_tokens)
        flops = chunks * 700_000_000
        return kernel(body, shape, (bias,), (block, *arrays), flops=flops, after=after)

    first = attend(q, 2, kvs[0], kvs[1])
    theirs = [attend(qs[0], 4, *kvs, after=(first,))]
    theirs.append(attend(qs[1], 4, *kvs, after=theirs))
    back = [shifted(theirs[0], "x", -1), shifted(theirs[1], "x", -2)]
    theirs.append(attend(qs[2], 4, *kvs, after=theirs[1:] + back[:1]))
    back.append(shifted(theirs[2], "x", -3))
    last = attend(q, 2, kvs[2], kvs[3], kvs[0], kvs[1], after=theirs[2:] + back[1:2])
    attended = kernel(merge_body, (block_tokens, VDIM), (), (first, last, *back))

    token_rows = lax.all_to_all(attended, "tp", split_axis=0, concat_axis=1, tiled=True)
    projected = jnp.dot(token_rows, out_rows, preferred_element_type=F32)
    return (latent.astype(F32) + modulations[2] * projected).astype(BF16)


def solution(mesh):
    split = Mesh(mesh.devices.reshape(4, 4, mesh.shape["tp"]), ("y", "x", "tp"))
    placed = (
        P(SP_TP, None),
        P(SP, None),
        P(),
        P(),
        P(None, SP, "tp"),
        P(),
        P("tp", None),
        P("tp", None),
        P(),
        P(),
        P(),
        P(None, "tp"),
        P(None, "tp"),
        P(None, "tp"),
        P(),
        P(),
        P("tp"),
        P("tp", None),
    )
    return jax.shard_map(
        shards, mesh=split, in_specs=placed, out_specs=P(SP_TP, None), check_vma=False
    )
```

```python
import functools
import math

import jax
import jax.numpy as jnp
from jax import lax
from jax.experimental import pallas as pl
from jax.experimental.pallas import tpu as pltpu
from jax.sharding import Mesh
from jax.sharding import PartitionSpec as P

NOPE = 64
ROPE = 32
HEAD = NOPE + ROPE
VDIM = 64
GRID_W = 64
TOK_DEV = 1024
CTX_DEV = 32
QRANK = 768
KVRANK = 512
CTX_PAD = 128
SP = ("y", "x")
SP_TP = ("y", "x", "tp")
BF16 = jnp.bfloat16
F32 = jnp.float32


epsilon = 1e-06
theta = 10000.0
SCALE = HEAD**-0.5 * math.log2(math.e)


def gathered(block, axis):
    count = lax.axis_size(axis)
    sent = jnp.broadcast_to(block[None], (count,) + block.shape)
    return lax.all_to_all(sent, axis, 0, 0, tiled=True)


def shifted(block, axis, step):
    count = lax.axis_size(axis)
    return lax.ppermute(block, axis, [(i, (i + step) % count) for i in range(count)])


def rope_tables(positions):
    pair_count = ROPE // 4
    frequency = jnp.power(theta, -jnp.arange(pair_count, dtype=F32) / pair_count)[:, None]
    row_angle = (positions // GRID_W).astype(F32)[None, :] * frequency
    col_angle = (positions % GRID_W).astype(F32)[None, :] * frequency
    return jnp.concatenate(
        [jnp.cos(row_angle), jnp.sin(row_angle), jnp.cos(col_angle), jnp.sin(col_angle)], axis=0
    )


def nt(a, b):
    return lax.dot_general(a, b, (((1,), (1,)), ((), ())), preferred_element_type=F32)


def tn(a, b):
    return lax.dot_general(a, b, (((0,), (0,)), ((), ())), preferred_element_type=F32)


def head_norm(u, gain):
    scale = lax.rsqrt(jnp.sum(u * u, axis=0, keepdims=True) * (1.0 / HEAD) + epsilon)
    return u * scale * gain


def rotated(n, tables):
    a, b, c, d = (n[NOPE + 8 * i : NOPE + 8 * i + 8] for i in range(4))
    cos_r, sin_r, cos_c, sin_c = (tables[8 * i : 8 * i + 8] for i in range(4))
    return jnp.concatenate(
        [
            n[:NOPE],
            a * cos_r - b * sin_r,
            b * cos_r + a * sin_r,
            c * cos_c - d * sin_c,
            d * cos_c + c * sin_c,
        ],
        axis=0,
    )


def make_body(
    place_ref, all_hbm, ctx_ref, mod_ref, ngain_ref, lgain_ref, rope_ref, upq_ref, upk_ref,
    upv_ref, qgain_ref, kgain_ref, tab_ref, kv_ref, q_ref, *scratch
):
    raw, down, normed, sems = scratch
    width = down.shape[1]
    half = raw.shape[1]
    groups = 4
    rows = raw.shape[0] // groups
    copies = [
        pltpu.make_async_copy(
            all_hbm.at[g * rows : (g + 1) * rows, width:],
            raw.at[g * rows : (g + 1) * rows],
            sems.at[g],
        )
        for g in range(groups)
    ]
    copies.append(pltpu.make_async_copy(all_hbm.at[:, :width], down, sems.at[groups]))
    for copy in copies:
        copy.start()
    tokens = normed.shape[0]
    norm_gain = ngain_ref[...]

    def inverse(total):
        return lax.rsqrt(total * (1.0 / (2 * half)) + epsilon)

    factor = norm_gain * (1.0 + mod_ref[4:5])
    wide = ctx_ref[...].astype(F32)
    scale = inverse(jnp.sum(wide * wide, axis=1, keepdims=True))
    ctx_normed = (wide * scale * factor + mod_ref[3:4]).astype(BF16)

    factor = norm_gain * (1.0 + mod_ref[1:2])
    own = tokens // 16
    for g in range(groups):
        copies[g].wait()

        @pl.loop(g * (16 // groups), (g + 1) * (16 // groups))
        def _(t):
            start = pl.multiple_of(t * 2 * own, 2 * own)
            left = raw[pl.ds(start, own), :].astype(F32)
            right = raw[pl.ds(start + own, own), :].astype(F32)
            total = jnp.sum(left * left + right * right, axis=1, keepdims=True)
            scale = inverse(total)
            at = pl.ds(pl.multiple_of(t * own, own), own)
            shift = mod_ref[0:1]
            normed[at, :half] = (left * scale * factor[:, :half] + shift[:, :half]).astype(BF16)
            normed[at, half:] = (right * scale * factor[:, half:] + shift[:, half:]).astype(BF16)

    copies[groups].wait()

    def latent(u, gain):
        scale = lax.rsqrt(jnp.mean(u * u, axis=1, keepdims=True) + epsilon)
        return (u * scale * gain).astype(BF16)

    def keys_of(x):
        lat = latent(
            jnp.dot(x, down[:, QRANK:], preferred_element_type=F32), lgain_ref[:, QRANK:]
        )
        turned = nt(rope_ref[...], x).astype(BF16).astype(F32)
        key = head_norm(
            jnp.concatenate([nt(upk_ref[...], lat), turned], axis=0), kgain_ref[...]
        )
        return key, nt(upv_ref[...], lat).astype(BF16)

    key, value = keys_of(ctx_normed)
    made = jnp.concatenate([key.astype(BF16), value], axis=0)
    shape = (CTX_DEV, CTX_PAD)
    target = lax.broadcasted_iota(jnp.int32, shape, 0) + place_ref[0] * CTX_DEV
    spread = lax.broadcasted_iota(jnp.int32, shape, 1) == target
    spread = jnp.where(spread, 1.0, 0.0).astype(BF16)
    kv_ref[:, tokens:] = jnp.dot(made, spread, preferred_element_type=F32).astype(BF16)

    block = 256

    @pl.loop(0, tokens // block)
    def _(i):
        at = pl.ds(pl.multiple_of(i * block, block), block)
        x = normed[at, :]
        tables = tab_ref[:, at]
        key, value = keys_of(x)
        kv_ref[:HEAD, at] = rotated(key, tables).astype(BF16)
        kv_ref[HEAD:, at] = value
        lat = latent(
            jnp.dot(x, down[:, :QRANK], preferred_element_type=F32), lgain_ref[:, :QRANK]
        )
        t = head_norm(nt(upq_ref[...], lat), qgain_ref[...])
        q_ref[:, at] = rotated(t, tables).astype(BF16)


def attend_body(bias_ref, q_ref, *refs, chunks, span, ahead, block):
    kv_refs, out_ref = refs[:-1], refs[-1]
    tokens = q_ref.shape[1]
    ones = jnp.ones((16, span), BF16)
    spans = [(r, a) for r in kv_refs[:chunks] for a in range(0, tokens, span)]
    if len(kv_refs) == 4:
        ctx = functools.reduce(lambda s, r: s + r[:, tokens:].astype(F32), kv_refs, 0.0)
        ctx = ctx.astype(BF16)
        spans.append((None, 0))

    @pl.loop(0, tokens // block)
    def _(i):
        at = pl.ds(pl.multiple_of(i * block, block), block)
        q = q_ref[:, at]

        def scores(j):
            ref, a = spans[j]
            key = ctx[:HEAD] if ref is None else ref[:HEAD, a : a + span]
            s = tn(key, q) * SCALE
            return s + bias_ref[0] if ref is None else s

        def summands(j):
            ref, a = spans[j]
            value = ctx[HEAD:] if ref is None else ref[HEAD:, a : a + span]
            return jnp.concatenate([value, ones[:, : value.shape[1]]], axis=0)

        top = acc = None
        coming = [scores(j) for j in range(min(ahead, len(spans)))]
        for j in range(len(spans)):
            s = coming.pop(0)
            here = jnp.max(s, axis=0, keepdims=True)
            if j + ahead < len(spans):
                coming.append(scores(j + ahead))
            new_top = here if top is None else jnp.maximum(top, here)
            weights = jnp.exp2(s - new_top).astype(BF16)
            add = jnp.dot(summands(j), weights, preferred_element_type=F32)
            acc = add if acc is None else acc * jnp.exp2(top - new_top) + add
            top = new_top
        total = acc[VDIM : VDIM + 1]
        out_ref[:VDIM, at] = (acc[:VDIM] / total).astype(BF16)
        lse = top + jnp.log2(total)
        hi = lse.astype(BF16).astype(F32)
        mid = (lse - hi).astype(BF16).astype(F32)
        low = lse - hi - mid
        zeros = jnp.zeros((13, block), F32)
        out_ref[VDIM:, at] = jnp.concatenate([hi, mid, low, zeros], axis=0).astype(BF16)


def merge_body(*refs):
    parts, out_ref = refs[:-1], refs[-1]
    lses, outs = [], []
    for r in parts:
        tail = r[VDIM:, :].astype(F32)
        lses.append(tail[0:1] + tail[1:2] + tail[2:3])
        outs.append(r[:VDIM, :].astype(F32))
    top = functools.reduce(jnp.maximum, lses)
    weights = [jnp.exp2(s - top) for s in lses]
    total = functools.reduce(jnp.add, weights)
    acc = functools.reduce(jnp.add, [w * o for w, o in zip(weights, outs)])
    out_ref[...] = (acc / total).T.astype(BF16)


def kernel(body, shape, scalars, arrays, flops=0, after=()):
    count = len(scalars) + len(arrays)
    ordered = tuple(after)

    def with_order(*refs):
        body(*refs[:count], refs[-1])

    vmem = pl.BlockSpec(memory_space=pltpu.VMEM)
    smem = pl.BlockSpec(memory_space=pltpu.SMEM)
    return pl.pallas_call(
        with_order,
        out_shape=jax.ShapeDtypeStruct(shape, BF16),
        in_specs=[smem] * len(scalars)
        + [vmem] * len(arrays)
        + [pl.BlockSpec(memory_space=pl.ANY)] * len(ordered),
        out_specs=vmem,
        cost_estimate=pl.CostEstimate(flops=flops, bytes_accessed=0, transcendentals=0),
        compiler_params=pltpu.CompilerParams(vmem_limit_bytes=28 << 20),
    )(*scalars, *arrays, *ordered)


def make_heads(place, gathered_all, tokens, *arrays):
    vmem = pl.BlockSpec(memory_space=pltpu.VMEM)
    hbm = pl.BlockSpec(memory_space=pltpu.HBM)
    smem = pl.BlockSpec(memory_space=pltpu.SMEM)
    rows, width = gathered_all.shape
    down_width = QRANK + KVRANK
    return pl.pallas_call(
        make_body,
        out_shape=(
            jax.ShapeDtypeStruct((HEAD + VDIM, tokens + CTX_PAD), BF16),
            jax.ShapeDtypeStruct((HEAD, tokens), BF16),
        ),
        in_specs=[smem, hbm] + [vmem] * len(arrays),
        out_specs=(vmem, vmem),
        scratch_shapes=[
            pltpu.VMEM((rows, width - down_width), BF16),
            pltpu.VMEM((rows, down_width), BF16),
            pltpu.VMEM((tokens, 2 * (width - down_width)), BF16),
            pltpu.SemaphoreType.DMA((5,)),
        ],
        cost_estimate=pl.CostEstimate(flops=6_000_000_000, bytes_accessed=0, transcendentals=0),
        compiler_params=pltpu.CompilerParams(vmem_limit_bytes=58 << 20),
    )(place, gathered_all, *arrays)


def shards(
    latent,
    context,
    cond,
    cond_context,
    mod_weight,
    norm_gain,
    down_q,
    down_kv,
    rope_weight,
    qlat_gain,
    kvlat_gain,
    up_query,
    up_key,
    up_value,
    query_gain,
    key_gain,
    context_bias,
    out_weight,
):
    seq_index = lax.axis_index(SP)
    tp_count = lax.axis_size("tp")
    own_rows = latent.shape[0]
    block_tokens = own_rows * tp_count
    row_span = mod_weight.shape[1]
    features = latent.shape[1]
    halves = jnp.concatenate([latent[:, : features // 2], latent[:, features // 2 :]], axis=0)
    everything = lax.all_gather(
        jnp.concatenate([down_q, down_kv, halves], axis=1), "tp", axis=0, tiled=True
    )
    out_rows = lax.all_gather(out_weight, "tp", axis=0, tiled=True)

    activated = jax.nn.silu(jnp.stack([cond, cond_context]).astype(F32)).astype(BF16)
    own_part = lax.dynamic_slice_in_dim(activated, seq_index * row_span, row_span, 1)
    partial_value = jnp.concatenate(
        [
            jnp.einsum("d,rde->re", own_part[0], mod_weight, preferred_element_type=F32),
            jnp.einsum("d,rde->re", own_part[1], mod_weight[:2], preferred_element_type=F32),
            jnp.zeros((3, mod_weight.shape[2]), F32),
        ],
        axis=0,
    )
    summed = jnp.sum(gathered(partial_value, SP).reshape((-1,) + partial_value.shape), axis=0)
    modulations = jnp.swapaxes(gathered(summed, "tp").reshape((-1,) + summed.shape), 0, 1)
    modulations = modulations.reshape(summed.shape[0], -1)

    positions = seq_index * block_tokens + jnp.arange(block_tokens, dtype=jnp.int32)
    tables = rope_tables(positions)
    latent_gain = jnp.concatenate([qlat_gain, kvlat_gain]).astype(F32)
    kv, q = make_heads(
        lax.axis_index("y").astype(jnp.int32)[None],
        everything,
        block_tokens,
        context,
        modulations,
        norm_gain.astype(F32)[None, :],
        latent_gain[None, :],
        rope_weight.T,
        up_query.T,
        up_key.T,
        up_value.T,
        query_gain[:, None],
        key_gain[:, None],
        tables,
    )
    kvs = [kv] + [shifted(kv, "y", k) for k in range(1, 4)]
    qs = [shifted(q, "x", k) for k in range(1, 4)]
    bias = (context_bias + math.log(TOK_DEV / CTX_DEV)) * math.log2(math.e)

    def attend(block, chunks, *arrays, after=()):
        body = functools.partial(attend_body, chunks=chunks, span=256, ahead=2, block=512)
        shape = (VDIM + 16, block_tokens)
        flops = chunks * 700_000_000
        return kernel(body, shape, (bias,), (block, *arrays), flops=flops, after=after)

    first = attend(q, 2, kvs[0], kvs[1])
    theirs = [attend(qs[0], 4, *kvs, after=(first,))]
    theirs.append(attend(qs[1], 4, *kvs, after=theirs))
    back = [shifted(theirs[0], "x", -1), shifted(theirs[1], "x", -2)]
    theirs.append(attend(qs[2], 4, *kvs, after=theirs[1:] + back[:1]))
    back.append(shifted(theirs[2], "x", -3))
    last = attend(q, 2, kvs[2], kvs[3], kvs[0], kvs[1], after=theirs[2:] + back[1:2])
    attended = kernel(merge_body, (block_tokens, VDIM), (), (first, last, *back))

    token_rows = lax.all_to_all(attended, "tp", split_axis=0, concat_axis=1, tiled=True)
    projected = jnp.dot(token_rows, out_rows, preferred_element_type=F32)
    return (latent.astype(F32) + modulations[2] * projected).astype(BF16)


def solution(mesh):
    split = Mesh(mesh.devices.reshape(4, 4, mesh.shape["tp"]), ("y", "x", "tp"))
    placed = (
        P(SP_TP, None),
        P(SP, None),
        P(),
        P(),
        P(None, SP, "tp"),
        P(),
        P("tp", None),
        P("tp", None),
        P(),
        P(),
        P(),
        P(None, "tp"),
        P(None, "tp"),
        P(None, "tp"),
        P(),
        P(),
        P("tp"),
        P("tp", None),
    )
    return jax.shard_map(
        shards, mesh=split, in_specs=placed, out_specs=P(SP_TP, None), check_vma=False
    )
```

```python
import functools
import math

import jax
import jax.numpy as jnp
from jax import lax
from jax.experimental import pallas as pl
from jax.experimental.pallas import tpu as pltpu
from jax.sharding import Mesh
from jax.sharding import PartitionSpec as P

NOPE = 64
ROPE = 32
HEAD = NOPE + ROPE
VDIM = 64
GRID_W = 64
TOK_DEV = 1024
CTX_DEV = 32
QRANK = 768
KVRANK = 512
CTX_PAD = 128
SP = ("y", "x")
TP = ("zp", "zb", "c")
SP_TP = SP + TP
GROUP = ("x", "zb", "c")
BF16 = jnp.bfloat16
F32 = jnp.float32


epsilon = 1e-06
theta = 10000.0
SCALE = HEAD**-0.5 * math.log2(math.e)


def gathered(block, axis):
    count = lax.axis_size(axis)
    sent = jnp.broadcast_to(block[None], (count,) + block.shape)
    return lax.all_to_all(sent, axis, 0, 0, tiled=True)


def shifted(block, axis, step):
    count = lax.axis_size(axis)
    return lax.ppermute(block, axis, [(i, (i + step) % count) for i in range(count)])


def rope_tables(positions):
    pair_count = ROPE // 4
    frequency = jnp.power(theta, -jnp.arange(pair_count, dtype=F32) / pair_count)[:, None]
    row_angle = (positions // GRID_W).astype(F32)[None, :] * frequency
    col_angle = (positions % GRID_W).astype(F32)[None, :] * frequency
    return jnp.concatenate(
        [jnp.cos(row_angle), jnp.sin(row_angle), jnp.cos(col_angle), jnp.sin(col_angle)], axis=0
    )


def nt(a, b):
    return lax.dot_general(a, b, (((1,), (1,)), ((), ())), preferred_element_type=F32)


def tn(a, b):
    return lax.dot_general(a, b, (((0,), (0,)), ((), ())), preferred_element_type=F32)


def head_norm(u, gain):
    scale = lax.rsqrt(jnp.sum(u * u, axis=0, keepdims=True) * (1.0 / HEAD) + epsilon)
    return u * scale * gain


def rotated(n, tables):
    a, b, c, d = (n[NOPE + 8 * i : NOPE + 8 * i + 8] for i in range(4))
    cos_r, sin_r, cos_c, sin_c = (tables[8 * i : 8 * i + 8] for i in range(4))
    return jnp.concatenate(
        [
            n[:NOPE],
            a * cos_r - b * sin_r,
            b * cos_r + a * sin_r,
            c * cos_c - d * sin_c,
            d * cos_c + c * sin_c,
        ],
        axis=0,
    )


def make_body(
    place_ref, down_hbm, *refs
):
    raw_hbm, refs = refs[: len(PIECES)], refs[len(PIECES) :]
    (
        ctx_ref, mod_ref, ngain_ref, lgain_ref, rope_ref, up_ref, qgain_ref, kgain_ref, tab_ref,
        kv_ref, q_ref, raw, down, normed, sems,
    ) = refs
    starts = [sum(p[0] for p in PIECES[:n]) for n in range(len(PIECES))]
    own = raw.shape[0] // 16
    copies = [
        pltpu.make_async_copy(
            piece, raw.at[start * own : (start + count[0]) * own], sems.at[n]
        )
        for n, (piece, start, count) in enumerate(zip(raw_hbm, starts, PIECES))
    ]
    copies.append(pltpu.make_async_copy(down_hbm, down, sems.at[len(PIECES)]))
    for copy in copies:
        copy.start()
    tokens, width = normed.shape
    norm_gain = ngain_ref[...]
    upq = up_ref[:HEAD, :]
    upk = up_ref[HEAD : HEAD + NOPE, :KVRANK]
    upv = up_ref[HEAD + NOPE :, :KVRANK]

    def normal(wide, factor, shift):
        total = jnp.sum(wide * wide, axis=1, keepdims=True)
        scale = lax.rsqrt(total * (1.0 / width) + epsilon)
        return (wide * scale * factor + shift).astype(BF16)

    ctx_normed = normal(
        ctx_ref[...].astype(F32), norm_gain * (1.0 + mod_ref[4:5]), mod_ref[3:4]
    )
    factor = norm_gain * (1.0 + mod_ref[1:2])
    shift = mod_ref[0:1]
    for part in range(2):
        for copy in copies[part * len(PIECES) // 2 : (part + 1) * len(PIECES) // 2]:
            copy.wait()

        @pl.loop(8 * part, 8 * part + 8)
        def _(n):
            at = pl.ds(pl.multiple_of(place_ref[n] * own, own), own)
            here = pl.ds(pl.multiple_of(n * own, own), own)
            normed[at, :] = normal(raw[here, :].astype(F32), factor, shift)

    copies[len(PIECES)].wait()

    def latent(u, gain):
        scale = lax.rsqrt(jnp.mean(u * u, axis=1, keepdims=True) + epsilon)
        return (u * scale * gain).astype(BF16)

    def keys_of(x):
        lat = latent(
            jnp.dot(x, down[:, QRANK:], preferred_element_type=F32), lgain_ref[:, QRANK:]
        )
        turned = nt(rope_ref[...], x).astype(BF16).astype(F32)
        key = head_norm(
            jnp.concatenate([nt(upk, lat), turned], axis=0), kgain_ref[...]
        )
        return key, nt(upv, lat).astype(BF16)

    key, value = keys_of(ctx_normed)
    made = jnp.concatenate([key.astype(BF16), value], axis=0)
    shape = (CTX_DEV, CTX_PAD)
    target = lax.broadcasted_iota(jnp.int32, shape, 0) + place_ref[16] * CTX_DEV
    spread = lax.broadcasted_iota(jnp.int32, shape, 1) == target
    spread = jnp.where(spread, 1.0, 0.0).astype(BF16)
    kv_ref[:, tokens:] = jnp.dot(made, spread, preferred_element_type=F32).astype(BF16)

    block = 256

    @pl.loop(0, tokens // block)
    def _(i):
        at = pl.ds(pl.multiple_of(i * block, block), block)
        x = normed[at, :]
        tables = tab_ref[:, at]
        key, value = keys_of(x)
        kv_ref[:HEAD, at] = rotated(key, tables).astype(BF16)
        kv_ref[HEAD:, at] = value
        lat = latent(
            jnp.dot(x, down[:, :QRANK], preferred_element_type=F32), lgain_ref[:, :QRANK]
        )
        t = head_norm(nt(upq, lat), qgain_ref[...])
        q_ref[:, at] = rotated(t, tables).astype(BF16)


def attend_body(bias_ref, q_ref, *refs, chunks, span, ahead, block):
    kv_refs, out_ref = refs[:-1], refs[-1]
    tokens = q_ref.shape[1]
    ones = jnp.ones((16, span), BF16)
    spans = [(r, a) for r in kv_refs[:chunks] for a in range(0, tokens, span)]
    if len(kv_refs) == 4:
        ctx = functools.reduce(lambda s, r: s + r[:, tokens:].astype(F32), kv_refs, 0.0)
        ctx = ctx.astype(BF16)
        spans.append((None, 0))

    @pl.loop(0, tokens // block)
    def _(i):
        at = pl.ds(pl.multiple_of(i * block, block), block)
        q = q_ref[:, at]

        def scores(j):
            ref, a = spans[j]
            key = ctx[:HEAD] if ref is None else ref[:HEAD, a : a + span]
            s = tn(key, q) * SCALE
            return s + bias_ref[0] if ref is None else s

        def summands(j):
            ref, a = spans[j]
            value = ctx[HEAD:] if ref is None else ref[HEAD:, a : a + span]
            return jnp.concatenate([value, ones[:, : value.shape[1]]], axis=0)

        top = acc = None
        coming = [scores(j) for j in range(min(ahead, len(spans)))]
        for j in range(len(spans)):
            s = coming.pop(0)
            here = jnp.max(s, axis=0, keepdims=True)
            if j + ahead < len(spans):
                coming.append(scores(j + ahead))
            new_top = here if top is None else jnp.maximum(top, here)
            weights = jnp.exp2(s - new_top).astype(BF16)
            add = jnp.dot(summands(j), weights, preferred_element_type=F32)
            acc = add if acc is None else acc * jnp.exp2(top - new_top) + add
            top = new_top
        total = acc[VDIM : VDIM + 1]
        out_ref[:VDIM, at] = (acc[:VDIM] / total).astype(BF16)
        lse = top + jnp.log2(total)
        hi = lse.astype(BF16).astype(F32)
        mid = (lse - hi).astype(BF16).astype(F32)
        low = lse - hi - mid
        zeros = jnp.zeros((13, block), F32)
        out_ref[VDIM:, at] = jnp.concatenate([hi, mid, low, zeros], axis=0).astype(BF16)


def merge_body(*refs):
    parts, out_ref = refs[:-1], refs[-1]
    lses, outs = [], []
    for r in parts:
        tail = r[VDIM:, :].astype(F32)
        lses.append(tail[0:1] + tail[1:2] + tail[2:3])
        outs.append(r[:VDIM, :].astype(F32))
    top = functools.reduce(jnp.maximum, lses)
    weights = [jnp.exp2(s - top) for s in lses]
    total = functools.reduce(jnp.add, weights)
    acc = functools.reduce(jnp.add, [w * o for w, o in zip(weights, outs)])
    out_ref[...] = (acc / total).T.astype(BF16)


def join_body(first_ref, second_ref, out_ref):
    rows = first_ref.shape[0]
    out_ref[:rows, :] = first_ref[...]
    out_ref[rows:, :] = second_ref[...]


def held(arrays, until):
    count = len(arrays)
    anywhere = pl.BlockSpec(memory_space=pl.ANY)
    return pl.pallas_call(
        lambda *refs: None,
        out_shape=tuple(jax.ShapeDtypeStruct(a.shape, a.dtype) for a in arrays),
        in_specs=[anywhere] * (count + 1),
        out_specs=(anywhere,) * count,
        input_output_aliases={n: n for n in range(count)},
    )(*arrays, until)


def kernel(body, shape, scalars, arrays, flops=0, after=()):
    count = len(scalars) + len(arrays)
    ordered = tuple(after)

    def with_order(*refs):
        body(*refs[:count], refs[-1])

    vmem = pl.BlockSpec(memory_space=pltpu.VMEM)
    smem = pl.BlockSpec(memory_space=pltpu.SMEM)
    return pl.pallas_call(
        with_order,
        out_shape=jax.ShapeDtypeStruct(shape, BF16),
        in_specs=[smem] * len(scalars)
        + [vmem] * len(arrays)
        + [pl.BlockSpec(memory_space=pl.ANY)] * len(ordered),
        out_specs=vmem,
        cost_estimate=pl.CostEstimate(flops=flops, bytes_accessed=0, transcendentals=0),
        compiler_params=pltpu.CompilerParams(vmem_limit_bytes=28 << 20),
    )(*scalars, *arrays, *ordered)


PIECES = [
    (count, step, first, other)
    for other in (0, 1)
    for count, step, first in ((2, 0, 0), (2, 1, 0), (2, 3, 0), (1, 2, 0), (1, 2, 1))
]


def make_heads(place, down, pieces, *arrays):
    vmem = pl.BlockSpec(memory_space=pltpu.VMEM)
    hbm = pl.BlockSpec(memory_space=pltpu.HBM)
    smem = pl.BlockSpec(memory_space=pltpu.SMEM)
    tokens = sum(piece.shape[0] for piece in pieces)
    width = pieces[0].shape[1]
    return pl.pallas_call(
        make_body,
        out_shape=(
            jax.ShapeDtypeStruct((HEAD + VDIM, tokens + CTX_PAD), BF16),
            jax.ShapeDtypeStruct((HEAD, tokens), BF16),
        ),
        in_specs=[smem, hbm] + [hbm] * len(pieces) + [vmem] * len(arrays),
        out_specs=(vmem, vmem),
        scratch_shapes=[
            pltpu.VMEM((tokens, width), BF16),
            pltpu.VMEM(down.shape, BF16),
            pltpu.VMEM((tokens, width), BF16),
            pltpu.SemaphoreType.DMA((len(PIECES) + 1,)),
        ],
        cost_estimate=pl.CostEstimate(flops=6_000_000_000, bytes_accessed=0, transcendentals=0),
        compiler_params=pltpu.CompilerParams(vmem_limit_bytes=58 << 20),
    )(place, down, *pieces, *arrays)


def shards(
    latent,
    context,
    cond,
    cond_context,
    mod_weight,
    norm_gain,
    down_q,
    down_kv,
    rope_weight,
    qlat_gain,
    kvlat_gain,
    up_query,
    up_key,
    up_value,
    query_gain,
    key_gain,
    context_bias,
    out_weight,
):
    seq_index = lax.axis_index(SP)
    own_rows = latent.shape[0]
    block_tokens = own_rows * 16
    row_span = mod_weight.shape[1]
    down = lax.all_gather(
        jnp.concatenate([down_q, down_kv], axis=1), TP, axis=0, tiled=True
    )
    out_rows = lax.all_gather(out_weight, TP, axis=0, tiled=True)

    activated = jax.nn.silu(jnp.stack([cond, cond_context]).astype(F32)).astype(BF16)
    own_part = lax.dynamic_slice_in_dim(activated, seq_index * row_span, row_span, 1)
    partial_value = jnp.concatenate(
        [
            jnp.einsum("d,rde->re", own_part[0], mod_weight, preferred_element_type=F32),
            jnp.einsum("d,rde->re", own_part[1], mod_weight[:2], preferred_element_type=F32),
            jnp.zeros((3, mod_weight.shape[2]), F32),
        ],
        axis=0,
    )
    summed = jnp.sum(gathered(partial_value, SP).reshape((-1,) + partial_value.shape), axis=0)
    biased = jnp.concatenate(
        [summed[:5], jnp.broadcast_to(context_bias[:, None], (3, summed.shape[1]))], axis=0
    )
    modulations = jnp.swapaxes(gathered(biased, TP).reshape((-1,) + summed.shape), 0, 1)
    modulations = modulations.reshape(summed.shape[0], -1)

    y, x, zp, zb, c = (lax.axis_index(axis) for axis in SP_TP)
    pair = kernel(
        join_body, (2 * own_rows, latent.shape[1]), (), (latent, shifted(latent, "zb", 1)),
        after=(summed,),
    )
    left, right = shifted(pair, "x", 1), shifted(pair, "x", -1)
    pair, left, right = held((pair, left, right), modulations)
    top = shifted(left[:own_rows], "x", 1)
    bottom = shifted(right[own_rows:], "x", -1)
    pieces = [pair, left, right, top, bottom]
    pieces += [shifted(piece, "c", 1) for piece in pieces]

    members = [
        (x - step + 4) % 4 * 4 + (zb + first + n) % 2 * 2 + (c + other) % 2
        for count, step, first, other in PIECES
        for n in range(count)
    ]

    swap = [(a * 4 + b, b * 4 + a) for a in range(4) for b in range(4)]
    ups = jnp.concatenate(
        [
            up_query.T,
            jnp.pad(
                jnp.concatenate([up_key.T, up_value.T], axis=0), ((0, 0), (0, QRANK - KVRANK))
            ),
        ],
        axis=0,
    )
    ups = lax.ppermute(ups, ("x", "zp"), swap)
    context = lax.ppermute(context, ("x", "zp"), swap)

    index = jnp.arange(block_tokens, dtype=jnp.int32)
    member = index // own_rows
    positions = (y * 4 + member // 4) * block_tokens
    positions = positions + (zp * 4 + member % 4) * own_rows + index % own_rows
    tables = rope_tables(positions)
    latent_gain = jnp.concatenate([qlat_gain, kvlat_gain]).astype(F32)
    kv, q = make_heads(
        jnp.stack(members + [y]).astype(jnp.int32),
        down,
        pieces,
        context,
        modulations,
        norm_gain.astype(F32)[None, :],
        latent_gain[None, :],
        rope_weight.T,
        ups,
        query_gain[:, None],
        key_gain[:, None],
        tables,
    )
    kvs = [kv] + [shifted(kv, "y", k) for k in range(1, 4)]
    qs = [shifted(q, "zp", k) for k in (1, 2, 3)]
    heads = modulations[5].reshape(16, -1)[:, 0]
    bias = lax.dynamic_slice_in_dim(heads, lax.axis_index(GROUP), 1)
    bias = (bias + math.log(TOK_DEV / CTX_DEV)) * math.log2(math.e)

    def attend(block, chunks, *arrays, after=()):
        body = functools.partial(attend_body, chunks=chunks, span=256, ahead=2, block=512)
        shape = (VDIM + 16, block_tokens)
        flops = chunks * 700_000_000
        return kernel(body, shape, (bias,), (block, *arrays), flops=flops, after=after)

    first = attend(q, 2, kvs[0], kvs[1])
    theirs = [attend(qs[0], 4, *kvs, after=(first,))]
    theirs.append(attend(qs[1], 4, *kvs, after=theirs))
    back = [shifted(theirs[0], "zp", -1), shifted(theirs[1], "zp", -2)]
    theirs.append(attend(qs[2], 4, *kvs, after=theirs[1:] + back[:1]))
    back.append(shifted(theirs[2], "zp", -3))
    last = attend(q, 2, kvs[2], kvs[3], kvs[0], kvs[1], after=theirs[2:] + back[1:2])
    attended = kernel(merge_body, (block_tokens, VDIM), (), (first, last, *back))

    token_rows = lax.all_to_all(attended, GROUP, split_axis=0, concat_axis=1, tiled=True)
    projected = jnp.dot(token_rows, out_rows, preferred_element_type=F32)
    return (latent.astype(F32) + modulations[2] * projected).astype(BF16)


def solution(mesh):
    split = Mesh(mesh.devices.reshape(4, 4, 4, 2, 2), SP_TP)
    placed = (
        P(SP_TP, None),
        P(SP, None),
        P(),
        P(),
        P(None, SP, TP),
        P(),
        P(TP, None),
        P(TP, None),
        P(),
        P(),
        P(),
        P(None, TP),
        P(None, TP),
        P(None, TP),
        P(),
        P(),
        P(TP),
        P(TP, None),
    )
    return jax.shard_map(
        shards, mesh=split, in_specs=placed, out_specs=P(SP_TP, None), check_vma=False
    )
```

```python
import functools
import math

import jax
import jax.numpy as jnp
from jax import lax
from jax.experimental import pallas as pl
from jax.experimental.pallas import tpu as pltpu
from jax.sharding import Mesh
from jax.sharding import PartitionSpec as P

NOPE = 64
ROPE = 32
HEAD = NOPE + ROPE
VDIM = 64
GRID_W = 64
TOK_DEV = 1024
CTX_DEV = 32
QRANK = 768
KVRANK = 512
CTX_PAD = 128
GROUPS = 2
SP = ("y", "x")
SP_TP = ("y", "x", "tp")
BF16 = jnp.bfloat16
F32 = jnp.float32


epsilon = 1e-06
theta = 10000.0
SCALE = HEAD**-0.5 * math.log2(math.e)


def gathered(block, axis):
    count = lax.axis_size(axis)
    sent = jnp.broadcast_to(block[None], (count,) + block.shape)
    return lax.all_to_all(sent, axis, 0, 0, tiled=True)


def shifted(block, axis, step):
    count = lax.axis_size(axis)
    return lax.ppermute(block, axis, [(i, (i + step) % count) for i in range(count)])


def rope_tables(positions):
    pair_count = ROPE // 4
    frequency = jnp.power(theta, -jnp.arange(pair_count, dtype=F32) / pair_count)[:, None]
    row_angle = (positions // GRID_W).astype(F32)[None, :] * frequency
    col_angle = (positions % GRID_W).astype(F32)[None, :] * frequency
    return jnp.concatenate(
        [jnp.cos(row_angle), jnp.sin(row_angle), jnp.cos(col_angle), jnp.sin(col_angle)], axis=0
    )


def nt(a, b):
    return lax.dot_general(a, b, (((1,), (1,)), ((), ())), preferred_element_type=F32)


def tn(a, b):
    return lax.dot_general(a, b, (((0,), (0,)), ((), ())), preferred_element_type=F32)


def head_norm(u, gain):
    scale = lax.rsqrt(jnp.sum(u * u, axis=0, keepdims=True) * (1.0 / HEAD) + epsilon)
    return u * scale * gain


def rotated(n, tables):
    a, b, c, d = (n[NOPE + 8 * i : NOPE + 8 * i + 8] for i in range(4))
    cos_r, sin_r, cos_c, sin_c = (tables[8 * i : 8 * i + 8] for i in range(4))
    return jnp.concatenate(
        [
            n[:NOPE],
            a * cos_r - b * sin_r,
            b * cos_r + a * sin_r,
            c * cos_c - d * sin_c,
            d * cos_c + c * sin_c,
        ],
        axis=0,
    )


def make_body(
    place_ref, all_hbm, ctx_ref, mod_ref, ngain_ref, lgain_ref, rope_ref, upq_ref, upk_ref,
    upv_ref, qgain_ref, kgain_ref, tab_ref, kv_ref, q_ref, *scratch
):
    raw, down, normed, sems = scratch
    width = down.shape[1]
    half = raw.shape[1]
    groups = GROUPS
    rows = raw.shape[0] // groups
    tokens = raw.shape[0] // 2
    block = tokens // groups
    own = tokens // 16

    def group_copy(g):
        span = slice(g * rows, (g + 1) * rows)
        return pltpu.make_async_copy(all_hbm.at[span, width:], raw.at[span], sems.at[g])

    def down_copy(n, first, last):
        span = slice(first, last)
        return pltpu.make_async_copy(all_hbm.at[:, span], down.at[:, span], sems.at[groups + n])

    arrivals = [group_copy(g) for g in range(groups)]
    weights = [down_copy(0, QRANK, width), down_copy(1, 0, QRANK)]
    for copy in arrivals[:1] + weights + arrivals[1:]:
        copy.start()
    norm_gain = ngain_ref[...]

    def inverse(total):
        return lax.rsqrt(total * (1.0 / (2 * half)) + epsilon)

    factor = norm_gain * (1.0 + mod_ref[4:5])
    wide = ctx_ref[...].astype(F32)
    scale = inverse(jnp.sum(wide * wide, axis=1, keepdims=True))
    ctx_normed = (wide * scale * factor + mod_ref[3:4]).astype(BF16)

    factor = norm_gain * (1.0 + mod_ref[1:2])
    shift = mod_ref[0:1]

    def normalise(g):
        arrivals[g].wait()
        for t in range(g * block // own, (g + 1) * block // own):
            left = raw[2 * t * own : (2 * t + 1) * own, :].astype(F32)
            right = raw[(2 * t + 1) * own : (2 * t + 2) * own, :].astype(F32)
            scale = inverse(jnp.sum(left * left + right * right, axis=1, keepdims=True))
            at = slice(t * own, (t + 1) * own)
            normed[at, :half] = (left * scale * factor[:, :half] + shift[:, :half]).astype(BF16)
            normed[at, half:] = (right * scale * factor[:, half:] + shift[:, half:]).astype(BF16)

    def latent(u, gain):
        scale = lax.rsqrt(jnp.mean(u * u, axis=1, keepdims=True) + epsilon)
        return (u * scale * gain).astype(BF16)

    def keys_of(x):
        lat = latent(
            jnp.dot(x, down[:, QRANK:], preferred_element_type=F32), lgain_ref[:, QRANK:]
        )
        turned = nt(rope_ref[...], x).astype(BF16).astype(F32)
        key = head_norm(
            jnp.concatenate([nt(upk_ref[...], lat), turned], axis=0), kgain_ref[...]
        )
        return key, nt(upv_ref[...], lat).astype(BF16)

    normalise(0)
    weights[0].wait()
    key, value = keys_of(ctx_normed)
    made = jnp.concatenate([key.astype(BF16), value], axis=0)
    shape = (CTX_DEV, CTX_PAD)
    target = lax.broadcasted_iota(jnp.int32, shape, 0) + place_ref[0] * CTX_DEV
    spread = lax.broadcasted_iota(jnp.int32, shape, 1) == target
    spread = jnp.where(spread, 1.0, 0.0).astype(BF16)
    kv_ref[:, tokens:] = jnp.dot(made, spread, preferred_element_type=F32).astype(BF16)
    weights[1].wait()
    for g in range(groups):
        at = slice(g * block, (g + 1) * block)
        x = normed[at, :]
        tables = tab_ref[:, at]
        key, value = keys_of(x)
        kv_ref[:HEAD, at] = rotated(key, tables).astype(BF16)
        kv_ref[HEAD:, at] = value
        if g + 1 < groups:
            normalise(g + 1)
        lat = latent(
            jnp.dot(x, down[:, :QRANK], preferred_element_type=F32), lgain_ref[:, :QRANK]
        )
        t = head_norm(nt(upq_ref[...], lat), qgain_ref[...])
        q_ref[:, at] = rotated(t, tables).astype(BF16)


def log_total(tail):
    tail = tail.astype(F32)
    return tail[0:1] + tail[1:2] + tail[2:3]


def attend_body(bias_ref, q_ref, *refs, chunks, span, ahead, block, resumed):
    kv_refs, out_ref = refs[:-1], refs[-1]
    if resumed:
        kv_refs, state_ref = kv_refs[:-1], kv_refs[-1]
    tokens = q_ref.shape[1]
    ones = jnp.ones((16, span), BF16)
    spans = [(r, a) for r in kv_refs[:chunks] for a in range(0, tokens, span)]
    if len(kv_refs) == 4:
        ctx = functools.reduce(lambda s, r: s + r[:, tokens:].astype(F32), kv_refs, 0.0)
        ctx = ctx.astype(BF16)
        spans.append((None, 0))

    @pl.loop(0, tokens // block)
    def _(i):
        at = pl.ds(pl.multiple_of(i * block, block), block)
        q = q_ref[:, at]

        def scores(j):
            ref, a = spans[j]
            key = ctx[:HEAD] if ref is None else ref[:HEAD, a : a + span]
            s = tn(key, q) * SCALE
            return s + bias_ref[0] if ref is None else s

        def summands(j):
            ref, a = spans[j]
            value = ctx[HEAD:] if ref is None else ref[HEAD:, a : a + span]
            return jnp.concatenate([value, ones[:, : value.shape[1]]], axis=0)

        top = acc = None
        if resumed:
            top = log_total(state_ref[VDIM:, at])
            one = jnp.where(lax.broadcasted_iota(jnp.int32, (16, block), 0) == 0, 1.0, 0.0)
            acc = jnp.concatenate([state_ref[:VDIM, at].astype(F32), one], axis=0)
        coming = [scores(j) for j in range(min(ahead, len(spans)))]
        for j in range(len(spans)):
            s = coming.pop(0)
            here = jnp.max(s, axis=0, keepdims=True)
            if j + ahead < len(spans):
                coming.append(scores(j + ahead))
            new_top = here if top is None else jnp.maximum(top, here)
            weights = jnp.exp2(s - new_top).astype(BF16)
            add = jnp.dot(summands(j), weights, preferred_element_type=F32)
            acc = add if acc is None else acc * jnp.exp2(top - new_top) + add
            top = new_top
        total = acc[VDIM : VDIM + 1]
        out_ref[:VDIM, at] = (acc[:VDIM] / total).astype(BF16)
        lse = top + jnp.log2(total)
        hi = lse.astype(BF16).astype(F32)
        mid = (lse - hi).astype(BF16).astype(F32)
        low = lse - hi - mid
        zeros = jnp.zeros((13, block), F32)
        out_ref[VDIM:, at] = jnp.concatenate([hi, mid, low, zeros], axis=0).astype(BF16)


def merge_body(*refs):
    parts, out_ref = refs[:-1], refs[-1]
    lses, outs = [], []
    for r in parts:
        lses.append(log_total(r[VDIM:, :]))
        outs.append(r[:VDIM, :].astype(F32))
    top = functools.reduce(jnp.maximum, lses)
    weights = [jnp.exp2(s - top) for s in lses]
    total = functools.reduce(jnp.add, weights)
    acc = functools.reduce(jnp.add, [w * o for w, o in zip(weights, outs)])
    out_ref[...] = (acc / total).T.astype(BF16)


def kernel(body, shape, scalars, arrays, flops=0, after=()):
    count = len(scalars) + len(arrays)
    ordered = tuple(after)

    def with_order(*refs):
        body(*refs[:count], refs[-1])

    vmem = pl.BlockSpec(memory_space=pltpu.VMEM)
    smem = pl.BlockSpec(memory_space=pltpu.SMEM)
    return pl.pallas_call(
        with_order,
        out_shape=jax.ShapeDtypeStruct(shape, BF16),
        in_specs=[smem] * len(scalars)
        + [vmem] * len(arrays)
        + [pl.BlockSpec(memory_space=pl.ANY)] * len(ordered),
        out_specs=vmem,
        cost_estimate=pl.CostEstimate(flops=flops, bytes_accessed=0, transcendentals=0),
        compiler_params=pltpu.CompilerParams(vmem_limit_bytes=28 << 20),
    )(*scalars, *arrays, *ordered)


def make_heads(place, gathered_all, tokens, *arrays):
    vmem = pl.BlockSpec(memory_space=pltpu.VMEM)
    hbm = pl.BlockSpec(memory_space=pltpu.HBM)
    smem = pl.BlockSpec(memory_space=pltpu.SMEM)
    rows, width = gathered_all.shape
    down_width = QRANK + KVRANK
    return pl.pallas_call(
        make_body,
        out_shape=(
            jax.ShapeDtypeStruct((HEAD + VDIM, tokens + CTX_PAD), BF16),
            jax.ShapeDtypeStruct((HEAD, tokens), BF16),
        ),
        in_specs=[smem, hbm] + [vmem] * len(arrays),
        out_specs=(vmem, vmem),
        scratch_shapes=[
            pltpu.VMEM((rows, width - down_width), BF16),
            pltpu.VMEM((rows, down_width), BF16),
            pltpu.VMEM((tokens, 2 * (width - down_width)), BF16),
            pltpu.SemaphoreType.DMA((GROUPS + 2,)),
        ],
        cost_estimate=pl.CostEstimate(flops=6_000_000_000, bytes_accessed=0, transcendentals=0),
        compiler_params=pltpu.CompilerParams(vmem_limit_bytes=50 << 20),
    )(place, gathered_all, *arrays)


def shards(
    latent,
    context,
    cond,
    cond_context,
    mod_weight,
    norm_gain,
    down_q,
    down_kv,
    rope_weight,
    qlat_gain,
    kvlat_gain,
    up_query,
    up_key,
    up_value,
    query_gain,
    key_gain,
    context_bias,
    out_weight,
):
    seq_index = lax.axis_index(SP)
    tp_count = lax.axis_size("tp")
    own_rows = latent.shape[0]
    block_tokens = own_rows * tp_count
    row_span = mod_weight.shape[1]
    features = latent.shape[1]
    halves = jnp.concatenate([latent[:, : features // 2], latent[:, features // 2 :]], axis=0)
    everything = lax.all_gather(
        jnp.concatenate([down_q, down_kv, halves], axis=1), "tp", axis=0, tiled=True
    )
    out_rows = lax.all_gather(out_weight, "tp", axis=0, tiled=True)

    activated = jax.nn.silu(jnp.stack([cond, cond_context]).astype(F32)).astype(BF16)
    own_part = lax.dynamic_slice_in_dim(activated, seq_index * row_span, row_span, 1)
    partial_value = jnp.concatenate(
        [
            jnp.einsum("d,rde->re", own_part[0], mod_weight, preferred_element_type=F32),
            jnp.einsum("d,rde->re", own_part[1], mod_weight[:2], preferred_element_type=F32),
            jnp.zeros((3, mod_weight.shape[2]), F32),
        ],
        axis=0,
    )
    summed = jnp.sum(gathered(partial_value, SP).reshape((-1,) + partial_value.shape), axis=0)
    modulations = jnp.swapaxes(gathered(summed, "tp").reshape((-1,) + summed.shape), 0, 1)
    modulations = modulations.reshape(summed.shape[0], -1)

    positions = seq_index * block_tokens + jnp.arange(block_tokens, dtype=jnp.int32)
    tables = rope_tables(positions)
    latent_gain = jnp.concatenate([qlat_gain, kvlat_gain]).astype(F32)
    kv, q = make_heads(
        lax.axis_index("y").astype(jnp.int32)[None],
        everything,
        block_tokens,
        context,
        modulations,
        norm_gain.astype(F32)[None, :],
        latent_gain[None, :],
        rope_weight.T,
        up_query.T,
        up_key.T,
        up_value.T,
        query_gain[:, None],
        key_gain[:, None],
        tables,
    )
    kvs = [kv] + [shifted(kv, "y", k) for k in range(1, 4)]
    qs = [shifted(q, "x", k) for k in range(1, 4)]
    bias = (context_bias + math.log(TOK_DEV / CTX_DEV)) * math.log2(math.e)

    def attend(block, chunks, *arrays, state=(), after=()):
        body = functools.partial(
            attend_body, chunks=chunks, span=256, ahead=2, block=512, resumed=len(state) > 0
        )
        shape = (VDIM + 16, block_tokens)
        flops = chunks * 700_000_000
        return kernel(body, shape, (bias,), (block, *arrays, *state), flops=flops, after=after)

    first = attend(q, 2, kvs[0], kvs[1])
    begun = attend(qs[0], 3, kvs[0], kvs[1], kvs[3], after=(first,))
    theirs = [attend(qs[0], 1, kvs[2], kvs[0], kvs[1], kvs[3], state=(begun,))]
    theirs.append(attend(qs[1], 4, *kvs, after=theirs))
    back = [shifted(theirs[0], "x", -1), shifted(theirs[1], "x", -2)]
    theirs.append(attend(qs[2], 4, *kvs, after=theirs[1:] + back[:1]))
    back.append(shifted(theirs[2], "x", -3))
    last = attend(q, 2, kvs[2], kvs[3], kvs[0], kvs[1], after=theirs[2:] + back[1:2])
    attended = kernel(merge_body, (block_tokens, VDIM), (), (first, last, *back))

    token_rows = lax.all_to_all(attended, "tp", split_axis=0, concat_axis=1, tiled=True)
    projected = jnp.dot(token_rows, out_rows, preferred_element_type=F32)
    return (latent.astype(F32) + modulations[2] * projected).astype(BF16)


def solution(mesh):
    split = Mesh(mesh.devices.reshape(4, 4, mesh.shape["tp"]), ("y", "x", "tp"))
    placed = (
        P(SP_TP, None),
        P(SP, None),
        P(),
        P(),
        P(None, SP, "tp"),
        P(),
        P("tp", None),
        P("tp", None),
        P(),
        P(),
        P(),
        P(None, "tp"),
        P(None, "tp"),
        P(None, "tp"),
        P(),
        P(),
        P("tp"),
        P("tp", None),
    )
    return jax.shard_map(
        shards, mesh=split, in_specs=placed, out_specs=P(SP_TP, None), check_vma=False
    )
```

```python
import functools
import math

import jax
import jax.numpy as jnp
from jax import lax
from jax.experimental import pallas as pl
from jax.experimental.pallas import tpu as pltpu
from jax.sharding import Mesh
from jax.sharding import PartitionSpec as P

NOPE = 64
ROPE = 32
HEAD = NOPE + ROPE
VDIM = 64
GRID_W = 64
TOK_DEV = 1024
CTX_DEV = 32
QRANK = 768
KVRANK = 512
CTX_PAD = 128
GROUPS = 2
PARTS = 2
SP = ("y", "x")
SP_TP = ("y", "x", "tp")
BF16 = jnp.bfloat16
F32 = jnp.float32


epsilon = 1e-06
theta = 10000.0
SCALE = HEAD**-0.5 * math.log2(math.e)


def gathered(block, axis):
    count = lax.axis_size(axis)
    sent = jnp.broadcast_to(block[None], (count,) + block.shape)
    return lax.all_to_all(sent, axis, 0, 0, tiled=True)


def shifted(block, axis, step):
    count = lax.axis_size(axis)
    return lax.ppermute(block, axis, [(i, (i + step) % count) for i in range(count)])


def rope_tables(positions):
    pair_count = ROPE // 4
    frequency = jnp.power(theta, -jnp.arange(pair_count, dtype=F32) / pair_count)[:, None]
    row_angle = (positions // GRID_W).astype(F32)[None, :] * frequency
    col_angle = (positions % GRID_W).astype(F32)[None, :] * frequency
    return jnp.concatenate(
        [jnp.cos(row_angle), jnp.sin(row_angle), jnp.cos(col_angle), jnp.sin(col_angle)], axis=0
    )


def nt(a, b):
    return lax.dot_general(a, b, (((1,), (1,)), ((), ())), preferred_element_type=F32)


def tn(a, b):
    return lax.dot_general(a, b, (((0,), (0,)), ((), ())), preferred_element_type=F32)


def head_norm(u, gain):
    scale = lax.rsqrt(jnp.sum(u * u, axis=0, keepdims=True) * (1.0 / HEAD) + epsilon)
    return u * scale * gain


def rotated(n, tables):
    a, b, c, d = (n[NOPE + 8 * i : NOPE + 8 * i + 8] for i in range(4))
    cos_r, sin_r, cos_c, sin_c = (tables[8 * i : 8 * i + 8] for i in range(4))
    return jnp.concatenate(
        [
            n[:NOPE],
            a * cos_r - b * sin_r,
            b * cos_r + a * sin_r,
            c * cos_c - d * sin_c,
            d * cos_c + c * sin_c,
        ],
        axis=0,
    )


def latent_of(u, gain):
    scale = lax.rsqrt(jnp.mean(u * u, axis=1, keepdims=True) + epsilon)
    return (u * scale * gain).astype(BF16)


def key_body(
    place_ref, all_hbm, rope_ctx_ref, mod_ref, ngain_ref, lgain_ref, up_ref, kgain_ref, tab_ref,
    kv_ref, normed_hbm, raw, down, normed, sems
):
    half = raw.shape[1]
    groups = GROUPS
    rows = raw.shape[0] // groups
    tokens = raw.shape[0] // 2
    block = tokens // groups
    own = tokens // 16

    def group_copy(g):
        span = slice(g * rows, (g + 1) * rows)
        return pltpu.make_async_copy(all_hbm.at[span, QRANK + KVRANK :], raw.at[span], sems.at[g])

    arrivals = [group_copy(g) for g in range(groups)]
    weights = pltpu.make_async_copy(
        all_hbm.at[:, QRANK : QRANK + KVRANK], down, sems.at[groups]
    )
    onward = [
        pltpu.make_async_copy(
            normed.at[g * block : (g + 1) * block],
            normed_hbm.at[g * block : (g + 1) * block],
            sems.at[groups + 1 + g],
        )
        for g in range(groups)
    ]
    for copy in arrivals[:1] + [weights] + arrivals[1:]:
        copy.start()
    norm_gain = ngain_ref[...]

    def inverse(total):
        return lax.rsqrt(total * (1.0 / (2 * half)) + epsilon)

    factor = norm_gain * (1.0 + mod_ref[4:5])
    wide = rope_ctx_ref[ROPE:, :].astype(F32)
    scale = inverse(jnp.sum(wide * wide, axis=1, keepdims=True))
    ctx_normed = (wide * scale * factor + mod_ref[3:4]).astype(BF16)

    factor = norm_gain * (1.0 + mod_ref[1:2])
    shift = mod_ref[0:1]

    def normalise(g):
        arrivals[g].wait()
        for t in range(g * block // own, (g + 1) * block // own):
            left = raw[2 * t * own : (2 * t + 1) * own, :].astype(F32)
            right = raw[(2 * t + 1) * own : (2 * t + 2) * own, :].astype(F32)
            scale = inverse(jnp.sum(left * left + right * right, axis=1, keepdims=True))
            at = slice(t * own, (t + 1) * own)
            normed[at, :half] = (left * scale * factor[:, :half] + shift[:, :half]).astype(BF16)
            normed[at, half:] = (right * scale * factor[:, half:] + shift[:, half:]).astype(BF16)

    def keys_of(x):
        lat = latent_of(jnp.dot(x, down[...], preferred_element_type=F32), lgain_ref[...])
        turned = nt(rope_ctx_ref[:ROPE, :], x).astype(BF16).astype(F32)
        key = head_norm(
            jnp.concatenate([nt(up_ref[:NOPE, :], lat), turned], axis=0), kgain_ref[...]
        )
        return key, nt(up_ref[NOPE:, :], lat).astype(BF16)

    normalise(0)
    onward[0].start()
    weights.wait()
    key, value = keys_of(ctx_normed)
    made = jnp.concatenate([key.astype(BF16), value], axis=0)
    shape = (CTX_DEV, CTX_PAD)
    target = lax.broadcasted_iota(jnp.int32, shape, 0) + place_ref[0] * CTX_DEV
    spread = lax.broadcasted_iota(jnp.int32, shape, 1) == target
    spread = jnp.where(spread, 1.0, 0.0).astype(BF16)
    kv_ref[:, tokens:] = jnp.dot(made, spread, preferred_element_type=F32).astype(BF16)
    for g in range(groups):
        if g + 1 < groups:
            normalise(g + 1)
            onward[g + 1].start()
        at = slice(g * block, (g + 1) * block)
        key, value = keys_of(normed[at, :])
        kv_ref[:HEAD, at] = rotated(key, tab_ref[:, at]).astype(BF16)
        kv_ref[HEAD:, at] = value
    for copy in onward:
        copy.wait()


def query_body(
    normed_hbm, all_hbm, lgain_ref, upq_ref, qgain_ref, tab_ref, q_ref, normed, down, sems
):
    tokens, width = normed.shape
    block = tokens // 2
    part = width // PARTS
    blocks = [slice(g * block, (g + 1) * block) for g in range(2)]
    spans = [slice(n * part, (n + 1) * part) for n in range(PARTS)]
    tiles = [
        pltpu.make_async_copy(
            normed_hbm.at[blocks[0], span], normed.at[blocks[0], span], sems.at[n]
        )
        for n, span in enumerate(spans)
    ]
    weights = [
        pltpu.make_async_copy(all_hbm.at[span, :QRANK], down.at[span], sems.at[PARTS + n])
        for n, span in enumerate(spans)
    ]
    rest = pltpu.make_async_copy(
        normed_hbm.at[blocks[1]], normed.at[blocks[1]], sems.at[2 * PARTS]
    )
    for tile, weight in zip(tiles, weights):
        tile.start()
        weight.start()
    rest.start()

    def finish(u, at):
        lat = latent_of(u, lgain_ref[...])
        t = head_norm(nt(upq_ref[...], lat), qgain_ref[...])
        q_ref[:, at] = rotated(t, tab_ref[:, at]).astype(BF16)

    u = 0.0
    for n, span in enumerate(spans):
        tiles[n].wait()
        weights[n].wait()
        u = u + jnp.dot(
            normed[blocks[0], span], down[span, :], preferred_element_type=F32
        )
    rest.wait()
    v = jnp.dot(normed[blocks[1], :], down[...], preferred_element_type=F32)
    finish(u, blocks[0])
    finish(v, blocks[1])


def log_total(tail):
    tail = tail.astype(F32)
    return tail[0:1] + tail[1:2] + tail[2:3]


def attend_body(bias_ref, q_ref, *refs, chunks, span, ahead, block, resumed):
    kv_refs, out_ref = refs[:-1], refs[-1]
    if resumed:
        kv_refs, state_ref = kv_refs[:-1], kv_refs[-1]
    tokens = q_ref.shape[1]
    ones = jnp.ones((16, span), BF16)
    spans = [(r, a) for r in kv_refs[:chunks] for a in range(0, tokens, span)]
    if len(kv_refs) == 4:
        ctx = functools.reduce(lambda s, r: s + r[:, tokens:].astype(F32), kv_refs, 0.0)
        ctx = ctx.astype(BF16)
        spans.append((None, 0))

    @pl.loop(0, tokens // block)
    def _(i):
        at = pl.ds(pl.multiple_of(i * block, block), block)
        q = q_ref[:, at]

        def scores(j):
            ref, a = spans[j]
            key = ctx[:HEAD] if ref is None else ref[:HEAD, a : a + span]
            s = tn(key, q) * SCALE
            return s + bias_ref[0] if ref is None else s

        def summands(j):
            ref, a = spans[j]
            value = ctx[HEAD:] if ref is None else ref[HEAD:, a : a + span]
            return jnp.concatenate([value, ones[:, : value.shape[1]]], axis=0)

        top = acc = None
        if resumed:
            top = log_total(state_ref[VDIM:, at])
            one = jnp.where(lax.broadcasted_iota(jnp.int32, (16, block), 0) == 0, 1.0, 0.0)
            acc = jnp.concatenate([state_ref[:VDIM, at].astype(F32), one], axis=0)
        coming = [scores(j) for j in range(min(ahead, len(spans)))]
        for j in range(len(spans)):
            s = coming.pop(0)
            here = jnp.max(s, axis=0, keepdims=True)
            if j + ahead < len(spans):
                coming.append(scores(j + ahead))
            new_top = here if top is None else jnp.maximum(top, here)
            weights = jnp.exp2(s - new_top).astype(BF16)
            add = jnp.dot(summands(j), weights, preferred_element_type=F32)
            acc = add if acc is None else acc * jnp.exp2(top - new_top) + add
            top = new_top
        total = acc[VDIM : VDIM + 1]
        out_ref[:VDIM, at] = (acc[:VDIM] / total).astype(BF16)
        lse = top + jnp.log2(total)
        hi = lse.astype(BF16).astype(F32)
        mid = (lse - hi).astype(BF16).astype(F32)
        low = lse - hi - mid
        zeros = jnp.zeros((13, block), F32)
        out_ref[VDIM:, at] = jnp.concatenate([hi, mid, low, zeros], axis=0).astype(BF16)


def merge_body(*refs):
    parts, out_ref = refs[:-1], refs[-1]
    lses, outs = [], []
    for r in parts:
        lses.append(log_total(r[VDIM:, :]))
        outs.append(r[:VDIM, :].astype(F32))
    top = functools.reduce(jnp.maximum, lses)
    weights = [jnp.exp2(s - top) for s in lses]
    total = functools.reduce(jnp.add, weights)
    acc = functools.reduce(jnp.add, [w * o for w, o in zip(weights, outs)])
    out_ref[...] = (acc / total).T.astype(BF16)


def kernel(body, shape, scalars, arrays, flops=0, after=()):
    count = len(scalars) + len(arrays)
    ordered = tuple(after)

    def with_order(*refs):
        body(*refs[:count], refs[-1])

    vmem = pl.BlockSpec(memory_space=pltpu.VMEM)
    smem = pl.BlockSpec(memory_space=pltpu.SMEM)
    return pl.pallas_call(
        with_order,
        out_shape=jax.ShapeDtypeStruct(shape, BF16),
        in_specs=[smem] * len(scalars)
        + [vmem] * len(arrays)
        + [pl.BlockSpec(memory_space=pl.ANY)] * len(ordered),
        out_specs=vmem,
        cost_estimate=pl.CostEstimate(flops=flops, bytes_accessed=0, transcendentals=0),
        compiler_params=pltpu.CompilerParams(vmem_limit_bytes=28 << 20),
    )(*scalars, *arrays, *ordered)


def pack_body(down_q, down_kv, latent, out, sems):
    rows, half = latent.shape[0], latent.shape[1] // 2
    places = [
        (down_q, out.at[:, :QRANK]),
        (down_kv, out.at[:, QRANK : QRANK + KVRANK]),
        (latent.at[:, :half], out.at[:rows, QRANK + KVRANK :]),
        (latent.at[:, half:], out.at[rows:, QRANK + KVRANK :]),
    ]
    copies = [
        pltpu.make_async_copy(source, target, sems.at[n])
        for n, (source, target) in enumerate(places)
    ]
    for copy in copies:
        copy.start()
    for copy in copies:
        copy.wait()


def pack(down_q, down_kv, latent):
    hbm = pl.BlockSpec(memory_space=pltpu.HBM)
    vmem = pl.BlockSpec(memory_space=pltpu.VMEM)
    width = QRANK + KVRANK + latent.shape[1] // 2
    return pl.pallas_call(
        pack_body,
        out_shape=jax.ShapeDtypeStruct((2 * latent.shape[0], width), BF16),
        in_specs=[hbm] * 3,
        out_specs=vmem,
        scratch_shapes=[pltpu.SemaphoreType.DMA((4,))],
    )(down_q, down_kv, latent)


def make_keys(place, gathered_all, tokens, *arrays):
    vmem = pl.BlockSpec(memory_space=pltpu.VMEM)
    hbm = pl.BlockSpec(memory_space=pltpu.HBM)
    smem = pl.BlockSpec(memory_space=pltpu.SMEM)
    rows, width = gathered_all.shape
    half = width - QRANK - KVRANK
    return pl.pallas_call(
        key_body,
        out_shape=(
            jax.ShapeDtypeStruct((HEAD + VDIM, tokens + CTX_PAD), BF16),
            jax.ShapeDtypeStruct((tokens, 2 * half), BF16),
        ),
        in_specs=[smem, hbm] + [vmem] * len(arrays),
        out_specs=(vmem, hbm),
        scratch_shapes=[
            pltpu.VMEM((rows, half), BF16),
            pltpu.VMEM((rows, KVRANK), BF16),
            pltpu.VMEM((tokens, 2 * half), BF16),
            pltpu.SemaphoreType.DMA((2 * GROUPS + 1,)),
        ],
        cost_estimate=pl.CostEstimate(flops=3_000_000_000, bytes_accessed=0, transcendentals=0),
        compiler_params=pltpu.CompilerParams(vmem_limit_bytes=50 << 20),
    )(place, gathered_all, *arrays)


def make_queries(normed, gathered_all, *arrays):
    vmem = pl.BlockSpec(memory_space=pltpu.VMEM)
    hbm = pl.BlockSpec(memory_space=pltpu.HBM)
    tokens = normed.shape[0]
    return pl.pallas_call(
        query_body,
        out_shape=jax.ShapeDtypeStruct((HEAD, tokens), BF16),
        in_specs=[hbm, hbm] + [vmem] * len(arrays),
        out_specs=vmem,
        scratch_shapes=[
            pltpu.VMEM(normed.shape, BF16),
            pltpu.VMEM((normed.shape[1], QRANK), BF16),
            pltpu.SemaphoreType.DMA((2 * PARTS + 1,)),
        ],
        cost_estimate=pl.CostEstimate(flops=0, bytes_accessed=0, transcendentals=0),
        compiler_params=pltpu.CompilerParams(vmem_limit_bytes=56 << 20),
    )(normed, gathered_all, *arrays)


def shards(
    latent,
    context,
    cond,
    cond_context,
    mod_weight,
    norm_gain,
    down_q,
    down_kv,
    rope_weight,
    qlat_gain,
    kvlat_gain,
    up_query,
    up_key,
    up_value,
    query_gain,
    key_gain,
    context_bias,
    out_weight,
):
    seq_index = lax.axis_index(SP)
    tp_count = lax.axis_size("tp")
    own_rows = latent.shape[0]
    block_tokens = own_rows * tp_count
    row_span = mod_weight.shape[1]
    everything = lax.all_gather(pack(down_q, down_kv, latent), "tp", axis=0, tiled=True)
    out_rows = lax.all_gather(out_weight, "tp", axis=0, tiled=True)

    activated = jax.nn.silu(jnp.stack([cond, cond_context]).astype(F32)).astype(BF16)
    own_part = lax.dynamic_slice_in_dim(activated, seq_index * row_span, row_span, 1)
    partial_value = jnp.concatenate(
        [
            jnp.einsum("d,rde->re", own_part[0], mod_weight, preferred_element_type=F32),
            jnp.einsum("d,rde->re", own_part[1], mod_weight[:2], preferred_element_type=F32),
            jnp.zeros((3, mod_weight.shape[2]), F32),
        ],
        axis=0,
    )
    summed = jnp.sum(gathered(partial_value, SP).reshape((-1,) + partial_value.shape), axis=0)
    modulations = jnp.swapaxes(gathered(summed, "tp").reshape((-1,) + summed.shape), 0, 1)
    modulations = modulations.reshape(summed.shape[0], -1)

    positions = seq_index * block_tokens + jnp.arange(block_tokens, dtype=jnp.int32)
    tables = rope_tables(positions)
    kv, normed = make_keys(
        lax.axis_index("y").astype(jnp.int32)[None],
        everything,
        block_tokens,
        jnp.concatenate([rope_weight.T, context], axis=0),
        modulations,
        norm_gain.astype(F32)[None, :],
        kvlat_gain.astype(F32)[None, :],
        jnp.concatenate([up_key.T, up_value.T], axis=0),
        key_gain[:, None],
        tables,
    )
    kvs = [kv] + [shifted(kv, "y", k) for k in range(1, 4)]
    q = make_queries(
        normed,
        everything,
        qlat_gain.astype(F32)[None, :],
        up_query.T,
        query_gain[:, None],
        tables,
    )
    qs = [shifted(q, "x", k) for k in range(1, 4)]
    bias = (context_bias + math.log(TOK_DEV / CTX_DEV)) * math.log2(math.e)

    def attend(block, chunks, *arrays, state=(), after=()):
        body = functools.partial(
            attend_body, chunks=chunks, span=256, ahead=2, block=512, resumed=len(state) > 0
        )
        shape = (VDIM + 16, block_tokens)
        flops = chunks * 700_000_000
        return kernel(body, shape, (bias,), (block, *arrays, *state), flops=flops, after=after)

    first = attend(q, 2, kvs[0], kvs[1])
    begun = attend(qs[0], 3, *kvs[:3], after=(first,))
    theirs = [attend(qs[0], 1, kvs[3], *kvs[:3], state=(begun,))]
    theirs.append(attend(qs[1], 4, *kvs, after=theirs))
    back = [shifted(theirs[0], "x", -1), shifted(theirs[1], "x", -2)]
    theirs.append(attend(qs[2], 4, *kvs, after=theirs[1:] + back[:1]))
    back.append(shifted(theirs[2], "x", -3))
    last = attend(q, 2, kvs[2], kvs[3], kvs[0], kvs[1], after=theirs[2:] + back[1:2])
    attended = kernel(merge_body, (block_tokens, VDIM), (), (first, last, *back))

    token_rows = lax.all_to_all(attended, "tp", split_axis=0, concat_axis=1, tiled=True)
    projected = jnp.dot(token_rows, out_rows, preferred_element_type=F32)
    return (latent.astype(F32) + modulations[2] * projected).astype(BF16)


def solution(mesh):
    split = Mesh(mesh.devices.reshape(4, 4, mesh.shape["tp"]), ("y", "x", "tp"))
    placed = (
        P(SP_TP, None),
        P(SP, None),
        P(),
        P(),
        P(None, SP, "tp"),
        P(),
        P("tp", None),
        P("tp", None),
        P(),
        P(),
        P(),
        P(None, "tp"),
        P(None, "tp"),
        P(None, "tp"),
        P(),
        P(),
        P("tp"),
        P("tp", None),
    )
    return jax.shard_map(
        shards, mesh=split, in_specs=placed, out_specs=P(SP_TP, None), check_vma=False
    )
```

```python
import functools
import math

import jax
import jax.numpy as jnp
from jax import lax
from jax.experimental import pallas as pl
from jax.experimental.pallas import tpu as pltpu
from jax.sharding import Mesh
from jax.sharding import PartitionSpec as P

NOPE = 64
ROPE = 32
HEAD = NOPE + ROPE
VDIM = 64
GRID_W = 64
TOK_DEV = 1024
CTX_DEV = 32
QRANK = 768
KVRANK = 512
CTX_PAD = 128
GROUPS = 2
SP = ("y", "x")
SP_TP = ("y", "x", "tp")
BF16 = jnp.bfloat16
F32 = jnp.float32


epsilon = 1e-06
theta = 10000.0
SCALE = HEAD**-0.5 * math.log2(math.e)


def gathered(block, axis):
    count = lax.axis_size(axis)
    sent = jnp.broadcast_to(block[None], (count,) + block.shape)
    return lax.all_to_all(sent, axis, 0, 0, tiled=True)


def shifted(block, axis, step):
    count = lax.axis_size(axis)
    return lax.ppermute(block, axis, [(i, (i + step) % count) for i in range(count)])


def rope_tables(positions):
    pair_count = ROPE // 4
    frequency = jnp.power(theta, -jnp.arange(pair_count, dtype=F32) / pair_count)[:, None]
    row_angle = (positions // GRID_W).astype(F32)[None, :] * frequency
    col_angle = (positions % GRID_W).astype(F32)[None, :] * frequency
    return jnp.concatenate(
        [jnp.cos(row_angle), jnp.sin(row_angle), jnp.cos(col_angle), jnp.sin(col_angle)], axis=0
    )


def nt(a, b):
    return lax.dot_general(a, b, (((1,), (1,)), ((), ())), preferred_element_type=F32)


def tn(a, b):
    return lax.dot_general(a, b, (((0,), (0,)), ((), ())), preferred_element_type=F32)


def head_norm(u, gain):
    scale = lax.rsqrt(jnp.sum(u * u, axis=0, keepdims=True) * (1.0 / HEAD) + epsilon)
    return u * scale * gain


def rotated(n, tables):
    a, b, c, d = (n[NOPE + 8 * i : NOPE + 8 * i + 8] for i in range(4))
    cos_r, sin_r, cos_c, sin_c = (tables[8 * i : 8 * i + 8] for i in range(4))
    return jnp.concatenate(
        [
            n[:NOPE],
            a * cos_r - b * sin_r,
            b * cos_r + a * sin_r,
            c * cos_c - d * sin_c,
            d * cos_c + c * sin_c,
        ],
        axis=0,
    )


def make_body(
    place_ref, all_hbm, ctx_ref, mod_ref, ngain_ref, lgain_ref, rope_ref, upq_ref, upk_ref,
    upv_ref, qgain_ref, kgain_ref, tab_ref, kv_ref, q_ref, *scratch
):
    raw, down, normed, sems = scratch
    width = down.shape[1]
    half = raw.shape[1]
    groups = GROUPS
    rows = raw.shape[0] // groups
    tokens = raw.shape[0] // 2
    block = tokens // groups
    own = tokens // 16

    def group_copy(g):
        span = slice(g * rows, (g + 1) * rows)
        return pltpu.make_async_copy(all_hbm.at[span, width:], raw.at[span], sems.at[g])

    def down_copy(n, first, last):
        span = slice(first, last)
        return pltpu.make_async_copy(all_hbm.at[:, span], down.at[:, span], sems.at[groups + n])

    arrivals = [group_copy(g) for g in range(groups)]
    weights = [down_copy(0, QRANK, width), down_copy(1, 0, QRANK)]
    for copy in arrivals[:1] + weights + arrivals[1:]:
        copy.start()
    norm_gain = ngain_ref[...]

    def inverse(total):
        return lax.rsqrt(total * (1.0 / (2 * half)) + epsilon)

    factor = norm_gain * (1.0 + mod_ref[4:5])
    wide = ctx_ref[...].astype(F32)
    scale = inverse(jnp.sum(wide * wide, axis=1, keepdims=True))
    ctx_normed = (wide * scale * factor + mod_ref[3:4]).astype(BF16)

    factor = norm_gain * (1.0 + mod_ref[1:2])
    shift = mod_ref[0:1]

    def normalise(g):
        arrivals[g].wait()
        for t in range(g * block // own, (g + 1) * block // own):
            left = raw[2 * t * own : (2 * t + 1) * own, :].astype(F32)
            right = raw[(2 * t + 1) * own : (2 * t + 2) * own, :].astype(F32)
            scale = inverse(jnp.sum(left * left + right * right, axis=1, keepdims=True))
            at = slice(t * own, (t + 1) * own)
            normed[at, :half] = (left * scale * factor[:, :half] + shift[:, :half]).astype(BF16)
            normed[at, half:] = (right * scale * factor[:, half:] + shift[:, half:]).astype(BF16)

    def latent(u, gain):
        scale = lax.rsqrt(jnp.mean(u * u, axis=1, keepdims=True) + epsilon)
        return (u * scale * gain).astype(BF16)

    def keys_of(x):
        lat = latent(
            jnp.dot(x, down[:, QRANK:], preferred_element_type=F32), lgain_ref[:, QRANK:]
        )
        turned = nt(rope_ref[...], x).astype(BF16).astype(F32)
        key = head_norm(
            jnp.concatenate([nt(upk_ref[...], lat), turned], axis=0), kgain_ref[...]
        )
        return key, nt(upv_ref[...], lat).astype(BF16)

    normalise(0)
    weights[0].wait()
    key, value = keys_of(ctx_normed)
    made = jnp.concatenate([key.astype(BF16), value], axis=0)
    shape = (CTX_DEV, CTX_PAD)
    target = lax.broadcasted_iota(jnp.int32, shape, 0) + place_ref[0] * CTX_DEV
    spread = lax.broadcasted_iota(jnp.int32, shape, 1) == target
    spread = jnp.where(spread, 1.0, 0.0).astype(BF16)
    kv_ref[:, tokens:] = jnp.dot(made, spread, preferred_element_type=F32).astype(BF16)
    weights[1].wait()
    for g in range(groups):
        at = slice(g * block, (g + 1) * block)
        x = normed[at, :]
        tables = tab_ref[:, at]
        key, value = keys_of(x)
        kv_ref[:HEAD, at] = rotated(key, tables).astype(BF16)
        kv_ref[HEAD:, at] = value
        if g + 1 < groups:
            normalise(g + 1)
        lat = latent(
            jnp.dot(x, down[:, :QRANK], preferred_element_type=F32), lgain_ref[:, :QRANK]
        )
        t = head_norm(nt(upq_ref[...], lat), qgain_ref[...])
        q_ref[:, at] = rotated(t, tables).astype(BF16)


def log_total(tail):
    tail = tail.astype(F32)
    return tail[0:1] + tail[1:2] + tail[2:3]


def attend_body(bias_ref, q_ref, *refs, chunks, span, ahead, block, resumed):
    kv_refs, out_ref = refs[:-1], refs[-1]
    if resumed:
        kv_refs, state_ref = kv_refs[:-1], kv_refs[-1]
    tokens = q_ref.shape[1]
    ones = jnp.ones((16, span), BF16)
    spans = [(r, a) for r in kv_refs[:chunks] for a in range(0, tokens, span)]
    if len(kv_refs) == 4:
        ctx = functools.reduce(lambda s, r: s + r[:, tokens:].astype(F32), kv_refs, 0.0)
        ctx = ctx.astype(BF16)
        spans.append((None, 0))

    @pl.loop(0, tokens // block)
    def _(i):
        at = pl.ds(pl.multiple_of(i * block, block), block)
        q = q_ref[:, at]

        def scores(j):
            ref, a = spans[j]
            key = ctx[:HEAD] if ref is None else ref[:HEAD, a : a + span]
            s = tn(key, q) * SCALE
            return s + bias_ref[0] if ref is None else s

        def summands(j):
            ref, a = spans[j]
            value = ctx[HEAD:] if ref is None else ref[HEAD:, a : a + span]
            return jnp.concatenate([value, ones[:, : value.shape[1]]], axis=0)

        top = acc = None
        if resumed:
            top = log_total(state_ref[VDIM:, at])
            one = jnp.where(lax.broadcasted_iota(jnp.int32, (16, block), 0) == 0, 1.0, 0.0)
            acc = jnp.concatenate([state_ref[:VDIM, at].astype(F32), one], axis=0)
        coming = [scores(j) for j in range(min(ahead, len(spans)))]
        for j in range(len(spans)):
            s = coming.pop(0)
            here = jnp.max(s, axis=0, keepdims=True)
            if j + ahead < len(spans):
                coming.append(scores(j + ahead))
            new_top = here if top is None else jnp.maximum(top, here)
            weights = jnp.exp2(s - new_top).astype(BF16)
            add = jnp.dot(summands(j), weights, preferred_element_type=F32)
            acc = add if acc is None else acc * jnp.exp2(top - new_top) + add
            top = new_top
        total = acc[VDIM : VDIM + 1]
        out_ref[:VDIM, at] = (acc[:VDIM] / total).astype(BF16)
        lse = top + jnp.log2(total)
        hi = lse.astype(BF16).astype(F32)
        mid = (lse - hi).astype(BF16).astype(F32)
        low = lse - hi - mid
        zeros = jnp.zeros((13, block), F32)
        out_ref[VDIM:, at] = jnp.concatenate([hi, mid, low, zeros], axis=0).astype(BF16)


def merge_body(*refs):
    parts, out_ref = refs[:-1], refs[-1]
    lses, outs = [], []
    for r in parts:
        lses.append(log_total(r[VDIM:, :]))
        outs.append(r[:VDIM, :].astype(F32))
    top = functools.reduce(jnp.maximum, lses)
    weights = [jnp.exp2(s - top) for s in lses]
    total = functools.reduce(jnp.add, weights)
    acc = functools.reduce(jnp.add, [w * o for w, o in zip(weights, outs)])
    out_ref[...] = (acc / total).T.astype(BF16)


def kernel(body, shape, scalars, arrays, flops=0, after=()):
    count = len(scalars) + len(arrays)
    ordered = tuple(after)

    def with_order(*refs):
        body(*refs[:count], refs[-1])

    vmem = pl.BlockSpec(memory_space=pltpu.VMEM)
    smem = pl.BlockSpec(memory_space=pltpu.SMEM)
    return pl.pallas_call(
        with_order,
        out_shape=jax.ShapeDtypeStruct(shape, BF16),
        in_specs=[smem] * len(scalars)
        + [vmem] * len(arrays)
        + [pl.BlockSpec(memory_space=pl.ANY)] * len(ordered),
        out_specs=vmem,
        cost_estimate=pl.CostEstimate(flops=flops, bytes_accessed=0, transcendentals=0),
        compiler_params=pltpu.CompilerParams(vmem_limit_bytes=28 << 20),
    )(*scalars, *arrays, *ordered)


def pack_body(down_q, down_kv, latent, out, sems):
    rows, half = latent.shape[0], latent.shape[1] // 2
    places = [
        (down_q, out.at[:, :QRANK]),
        (down_kv, out.at[:, QRANK : QRANK + KVRANK]),
        (latent.at[:, :half], out.at[:rows, QRANK + KVRANK :]),
        (latent.at[:, half:], out.at[rows:, QRANK + KVRANK :]),
    ]
    copies = [
        pltpu.make_async_copy(source, target, sems.at[n])
        for n, (source, target) in enumerate(places)
    ]
    for copy in copies:
        copy.start()
    for copy in copies:
        copy.wait()


def pack(down_q, down_kv, latent):
    hbm = pl.BlockSpec(memory_space=pltpu.HBM)
    vmem = pl.BlockSpec(memory_space=pltpu.VMEM)
    width = QRANK + KVRANK + latent.shape[1] // 2
    return pl.pallas_call(
        pack_body,
        out_shape=jax.ShapeDtypeStruct((2 * latent.shape[0], width), BF16),
        in_specs=[hbm] * 3,
        out_specs=vmem,
        scratch_shapes=[pltpu.SemaphoreType.DMA((4,))],
    )(down_q, down_kv, latent)


def make_heads(place, gathered_all, tokens, *arrays):
    vmem = pl.BlockSpec(memory_space=pltpu.VMEM)
    hbm = pl.BlockSpec(memory_space=pltpu.HBM)
    smem = pl.BlockSpec(memory_space=pltpu.SMEM)
    rows, width = gathered_all.shape
    down_width = QRANK + KVRANK
    return pl.pallas_call(
        make_body,
        out_shape=(
            jax.ShapeDtypeStruct((HEAD + VDIM, tokens + CTX_PAD), BF16),
            jax.ShapeDtypeStruct((HEAD, tokens), BF16),
        ),
        in_specs=[smem, hbm] + [vmem] * len(arrays),
        out_specs=(vmem, vmem),
        scratch_shapes=[
            pltpu.VMEM((rows, width - down_width), BF16),
            pltpu.VMEM((rows, down_width), BF16),
            pltpu.VMEM((tokens, 2 * (width - down_width)), BF16),
            pltpu.SemaphoreType.DMA((GROUPS + 2,)),
        ],
        cost_estimate=pl.CostEstimate(flops=6_000_000_000, bytes_accessed=0, transcendentals=0),
        compiler_params=pltpu.CompilerParams(vmem_limit_bytes=50 << 20),
    )(place, gathered_all, *arrays)


def shards(
    latent,
    context,
    cond,
    cond_context,
    mod_weight,
    norm_gain,
    down_q,
    down_kv,
    rope_weight,
    qlat_gain,
    kvlat_gain,
    up_query,
    up_key,
    up_value,
    query_gain,
    key_gain,
    context_bias,
    out_weight,
):
    seq_index = lax.axis_index(SP)
    tp_count = lax.axis_size("tp")
    own_rows = latent.shape[0]
    block_tokens = own_rows * tp_count
    row_span = mod_weight.shape[1]
    everything = lax.all_gather(pack(down_q, down_kv, latent), "tp", axis=0, tiled=True)
    out_rows = lax.all_gather(out_weight, "tp", axis=0, tiled=True)

    activated = jax.nn.silu(jnp.stack([cond, cond_context]).astype(F32)).astype(BF16)
    own_part = lax.dynamic_slice_in_dim(activated, seq_index * row_span, row_span, 1)
    partial_value = jnp.concatenate(
        [
            jnp.einsum("d,rde->re", own_part[0], mod_weight, preferred_element_type=F32),
            jnp.einsum("d,rde->re", own_part[1], mod_weight[:2], preferred_element_type=F32),
            jnp.zeros((3, mod_weight.shape[2]), F32),
        ],
        axis=0,
    )
    summed = jnp.sum(gathered(partial_value, SP).reshape((-1,) + partial_value.shape), axis=0)
    modulations = jnp.swapaxes(gathered(summed, "tp").reshape((-1,) + summed.shape), 0, 1)
    modulations = modulations.reshape(summed.shape[0], -1)

    positions = seq_index * block_tokens + jnp.arange(block_tokens, dtype=jnp.int32)
    tables = rope_tables(positions)
    latent_gain = jnp.concatenate([qlat_gain, kvlat_gain]).astype(F32)
    kv, q = make_heads(
        lax.axis_index("y").astype(jnp.int32)[None],
        everything,
        block_tokens,
        context,
        modulations,
        norm_gain.astype(F32)[None, :],
        latent_gain[None, :],
        rope_weight.T,
        up_query.T,
        up_key.T,
        up_value.T,
        query_gain[:, None],
        key_gain[:, None],
        tables,
    )
    kvs = [kv] + [shifted(kv, "y", k) for k in range(1, 4)]
    qs = [shifted(q, "x", k) for k in range(1, 4)]
    bias = (context_bias + math.log(TOK_DEV / CTX_DEV)) * math.log2(math.e)

    def attend(block, chunks, *arrays, state=(), after=()):
        body = functools.partial(
            attend_body, chunks=chunks, span=256, ahead=2, block=512, resumed=len(state) > 0
        )
        shape = (VDIM + 16, block_tokens)
        flops = chunks * 50_000_000
        return kernel(body, shape, (bias,), (block, *arrays, *state), flops=flops, after=after)

    first = attend(q, 2, kvs[0], kvs[1])
    begun = attend(qs[0], 2, kvs[0], kvs[1], after=(first,))
    second = attend(qs[1], 2, kvs[0], kvs[1], after=(begun,))
    begun = attend(qs[0], 1, kvs[3], state=(begun,), after=(second,))
    theirs = [attend(qs[0], 1, kvs[2], kvs[0], kvs[1], kvs[3], state=(begun,))]
    theirs.append(
        attend(qs[1], 2, kvs[2], kvs[3], kvs[0], kvs[1], state=(second,), after=theirs)
    )
    back = [shifted(theirs[0], "x", -1), shifted(theirs[1], "x", -2)]
    theirs.append(attend(qs[2], 4, *kvs, after=theirs[1:] + back[:1]))
    back.append(shifted(theirs[2], "x", -3))
    last = attend(q, 2, kvs[2], kvs[3], kvs[0], kvs[1], after=theirs[2:] + back[1:2])
    attended = kernel(merge_body, (block_tokens, VDIM), (), (first, last, *back))

    token_rows = lax.all_to_all(attended, "tp", split_axis=0, concat_axis=1, tiled=True)
    projected = jnp.dot(token_rows, out_rows, preferred_element_type=F32)
    return (latent.astype(F32) + modulations[2] * projected).astype(BF16)


def solution(mesh):
    split = Mesh(mesh.devices.reshape(4, 4, mesh.shape["tp"]), ("y", "x", "tp"))
    placed = (
        P(SP_TP, None),
        P(SP, None),
        P(),
        P(),
        P(None, SP, "tp"),
        P(),
        P("tp", None),
        P("tp", None),
        P(),
        P(),
        P(),
        P(None, "tp"),
        P(None, "tp"),
        P(None, "tp"),
        P(),
        P(),
        P("tp"),
        P("tp", None),
    )
    return jax.shard_map(
        shards, mesh=split, in_specs=placed, out_specs=P(SP_TP, None), check_vma=False
    )
```

```python
import functools
import math

import jax
import jax.numpy as jnp
from jax import lax
from jax.experimental import pallas as pl
from jax.experimental.pallas import tpu as pltpu
from jax.sharding import Mesh
from jax.sharding import PartitionSpec as P

NOPE = 64
ROPE = 32
HEAD = NOPE + ROPE
VDIM = 64
GRID_W = 64
TOK_DEV = 1024
CTX_DEV = 32
QRANK = 768
KVRANK = 512
CTX_PAD = 128
GROUPS = 2
SP = ("y", "x")
SP_TP = ("y", "x", "tp")
BF16 = jnp.bfloat16
F32 = jnp.float32


epsilon = 1e-06
theta = 10000.0
SCALE = HEAD**-0.5 * math.log2(math.e)


def gathered(block, axis):
    count = lax.axis_size(axis)
    sent = jnp.broadcast_to(block[None], (count,) + block.shape)
    return lax.all_to_all(sent, axis, 0, 0, tiled=True)


def shifted(block, axis, step):
    count = lax.axis_size(axis)
    return lax.ppermute(block, axis, [(i, (i + step) % count) for i in range(count)])


def rope_tables(positions):
    pair_count = ROPE // 4
    frequency = jnp.power(theta, -jnp.arange(pair_count, dtype=F32) / pair_count)[:, None]
    row_angle = (positions // GRID_W).astype(F32)[None, :] * frequency
    col_angle = (positions % GRID_W).astype(F32)[None, :] * frequency
    return jnp.concatenate(
        [jnp.cos(row_angle), jnp.sin(row_angle), jnp.cos(col_angle), jnp.sin(col_angle)], axis=0
    )


def nt(a, b):
    return lax.dot_general(a, b, (((1,), (1,)), ((), ())), preferred_element_type=F32)


def tn(a, b):
    return lax.dot_general(a, b, (((0,), (0,)), ((), ())), preferred_element_type=F32)


def head_norm(u, gain):
    scale = lax.rsqrt(jnp.sum(u * u, axis=0, keepdims=True) * (1.0 / HEAD) + epsilon)
    return u * scale * gain


def rotated(n, tables):
    a, b, c, d = (n[NOPE + 8 * i : NOPE + 8 * i + 8] for i in range(4))
    cos_r, sin_r, cos_c, sin_c = (tables[8 * i : 8 * i + 8] for i in range(4))
    return jnp.concatenate(
        [
            n[:NOPE],
            a * cos_r - b * sin_r,
            b * cos_r + a * sin_r,
            c * cos_c - d * sin_c,
            d * cos_c + c * sin_c,
        ],
        axis=0,
    )


def make_body(
    place_ref, all_hbm, rope_ctx_ref, mod_ref, ngain_ref, lgain_ref, up_ref, qgain_ref, kgain_ref, tab_ref, kv_ref, q_ref, *scratch
):
    raw, down, normed, sems = scratch
    width = down.shape[1]
    half = raw.shape[1]
    groups = GROUPS
    rows = raw.shape[0] // groups
    tokens = raw.shape[0] // 2
    block = tokens // groups
    own = tokens // 16

    def group_copy(g):
        span = slice(g * rows, (g + 1) * rows)
        return pltpu.make_async_copy(all_hbm.at[span, width:], raw.at[span], sems.at[g])

    def down_copy(n, first, last):
        span = slice(first, last)
        return pltpu.make_async_copy(all_hbm.at[:, span], down.at[:, span], sems.at[groups + n])

    arrivals = [group_copy(g) for g in range(groups)]
    weights = [down_copy(0, QRANK, width), down_copy(1, 0, QRANK)]
    for copy in arrivals[:1] + weights + arrivals[1:]:
        copy.start()
    norm_gain = ngain_ref[...]

    def inverse(total):
        return lax.rsqrt(total * (1.0 / (2 * half)) + epsilon)

    factor = norm_gain * (1.0 + mod_ref[4:5])
    wide = rope_ctx_ref[ROPE:, :].astype(F32)
    scale = inverse(jnp.sum(wide * wide, axis=1, keepdims=True))
    ctx_normed = (wide * scale * factor + mod_ref[3:4]).astype(BF16)

    factor = norm_gain * (1.0 + mod_ref[1:2])
    shift = mod_ref[0:1]

    def normalise(g):
        arrivals[g].wait()
        for t in range(g * block // own, (g + 1) * block // own):
            left = raw[2 * t * own : (2 * t + 1) * own, :].astype(F32)
            right = raw[(2 * t + 1) * own : (2 * t + 2) * own, :].astype(F32)
            scale = inverse(jnp.sum(left * left + right * right, axis=1, keepdims=True))
            at = slice(t * own, (t + 1) * own)
            normed[at, :half] = (left * scale * factor[:, :half] + shift[:, :half]).astype(BF16)
            normed[at, half:] = (right * scale * factor[:, half:] + shift[:, half:]).astype(BF16)

    def latent(u, gain):
        scale = lax.rsqrt(jnp.mean(u * u, axis=1, keepdims=True) + epsilon)
        return (u * scale * gain).astype(BF16)

    def keys_of(x):
        lat = latent(
            jnp.dot(x, down[:, QRANK:], preferred_element_type=F32), lgain_ref[:, QRANK:]
        )
        turned = nt(rope_ctx_ref[:ROPE, :], x).astype(BF16).astype(F32)
        key = head_norm(
            jnp.concatenate([nt(up_ref[HEAD : HEAD + NOPE, :KVRANK], lat), turned], axis=0), kgain_ref[...]
        )
        return key, nt(up_ref[HEAD + NOPE :, :KVRANK], lat).astype(BF16)

    normalise(0)
    weights[0].wait()
    key, value = keys_of(ctx_normed)
    made = jnp.concatenate([key.astype(BF16), value], axis=0)
    shape = (CTX_DEV, CTX_PAD)
    target = lax.broadcasted_iota(jnp.int32, shape, 0) + place_ref[0] * CTX_DEV
    spread = lax.broadcasted_iota(jnp.int32, shape, 1) == target
    spread = jnp.where(spread, 1.0, 0.0).astype(BF16)
    kv_ref[:, tokens:] = jnp.dot(made, spread, preferred_element_type=F32).astype(BF16)
    weights[1].wait()
    for g in range(groups):
        at = slice(g * block, (g + 1) * block)
        x = normed[at, :]
        tables = tab_ref[:, at]
        key, value = keys_of(x)
        kv_ref[:HEAD, at] = rotated(key, tables).astype(BF16)
        kv_ref[HEAD:, at] = value
        if g + 1 < groups:
            normalise(g + 1)
        lat = latent(
            jnp.dot(x, down[:, :QRANK], preferred_element_type=F32), lgain_ref[:, :QRANK]
        )
        t = head_norm(nt(up_ref[:HEAD, :], lat), qgain_ref[...])
        q_ref[:, at] = rotated(t, tables).astype(BF16)


def log_total(tail):
    tail = tail.astype(F32)
    return tail[0:1] + tail[1:2] + tail[2:3]


def attend_body(bias_ref, q_ref, *refs, chunks, span, ahead, block, resumed):
    kv_refs, out_ref = refs[:-1], refs[-1]
    if resumed:
        kv_refs, state_ref = kv_refs[:-1], kv_refs[-1]
    tokens = q_ref.shape[1]
    ones = jnp.ones((16, span), BF16)
    spans = [(r, a) for r in kv_refs[:chunks] for a in range(0, tokens, span)]
    if len(kv_refs) == 4:
        ctx = functools.reduce(lambda s, r: s + r[:, tokens:].astype(F32), kv_refs, 0.0)
        ctx = ctx.astype(BF16)
        spans.append((None, 0))

    @pl.loop(0, tokens // block)
    def _(i):
        at = pl.ds(pl.multiple_of(i * block, block), block)
        q = q_ref[:, at]

        def scores(j):
            ref, a = spans[j]
            key = ctx[:HEAD] if ref is None else ref[:HEAD, a : a + span]
            s = tn(key, q) * SCALE
            return s + bias_ref[0] if ref is None else s

        def summands(j):
            ref, a = spans[j]
            value = ctx[HEAD:] if ref is None else ref[HEAD:, a : a + span]
            return jnp.concatenate([value, ones[:, : value.shape[1]]], axis=0)

        top = acc = None
        if resumed:
            top = log_total(state_ref[VDIM:, at])
            one = jnp.where(lax.broadcasted_iota(jnp.int32, (16, block), 0) == 0, 1.0, 0.0)
            acc = jnp.concatenate([state_ref[:VDIM, at].astype(F32), one], axis=0)
        coming = [scores(j) for j in range(min(ahead, len(spans)))]
        for j in range(len(spans)):
            s = coming.pop(0)
            here = jnp.max(s, axis=0, keepdims=True)
            if j + ahead < len(spans):
                coming.append(scores(j + ahead))
            new_top = here if top is None else jnp.maximum(top, here)
            weights = jnp.exp2(s - new_top).astype(BF16)
            add = jnp.dot(summands(j), weights, preferred_element_type=F32)
            acc = add if acc is None else acc * jnp.exp2(top - new_top) + add
            top = new_top
        total = acc[VDIM : VDIM + 1]
        out_ref[:VDIM, at] = (acc[:VDIM] / total).astype(BF16)
        lse = top + jnp.log2(total)
        hi = lse.astype(BF16).astype(F32)
        mid = (lse - hi).astype(BF16).astype(F32)
        low = lse - hi - mid
        zeros = jnp.zeros((13, block), F32)
        out_ref[VDIM:, at] = jnp.concatenate([hi, mid, low, zeros], axis=0).astype(BF16)


def merge_body(*refs):
    parts, out_ref = refs[:-1], refs[-1]
    lses, outs = [], []
    for r in parts:
        lses.append(log_total(r[VDIM:, :]))
        outs.append(r[:VDIM, :].astype(F32))
    top = functools.reduce(jnp.maximum, lses)
    weights = [jnp.exp2(s - top) for s in lses]
    total = functools.reduce(jnp.add, weights)
    acc = functools.reduce(jnp.add, [w * o for w, o in zip(weights, outs)])
    out_ref[...] = (acc / total).T.astype(BF16)


def kernel(body, shape, scalars, arrays, flops=0, after=()):
    count = len(scalars) + len(arrays)
    ordered = tuple(after)

    def with_order(*refs):
        body(*refs[:count], refs[-1])

    vmem = pl.BlockSpec(memory_space=pltpu.VMEM)
    smem = pl.BlockSpec(memory_space=pltpu.SMEM)
    return pl.pallas_call(
        with_order,
        out_shape=jax.ShapeDtypeStruct(shape, BF16),
        in_specs=[smem] * len(scalars)
        + [vmem] * len(arrays)
        + [pl.BlockSpec(memory_space=pl.ANY)] * len(ordered),
        out_specs=vmem,
        cost_estimate=pl.CostEstimate(flops=flops, bytes_accessed=0, transcendentals=0),
        compiler_params=pltpu.CompilerParams(vmem_limit_bytes=28 << 20),
    )(*scalars, *arrays, *ordered)


def pack_body(down_q, down_kv, latent, out, sems):
    rows, half = latent.shape[0], latent.shape[1] // 2
    places = [
        (down_q, out.at[:, :QRANK]),
        (down_kv, out.at[:, QRANK : QRANK + KVRANK]),
        (latent.at[:, :half], out.at[:rows, QRANK + KVRANK :]),
        (latent.at[:, half:], out.at[rows:, QRANK + KVRANK :]),
    ]
    copies = [
        pltpu.make_async_copy(source, target, sems.at[n])
        for n, (source, target) in enumerate(places)
    ]
    for copy in copies:
        copy.start()
    for copy in copies:
        copy.wait()


def pack(down_q, down_kv, latent):
    hbm = pl.BlockSpec(memory_space=pltpu.HBM)
    vmem = pl.BlockSpec(memory_space=pltpu.VMEM)
    width = QRANK + KVRANK + latent.shape[1] // 2
    return pl.pallas_call(
        pack_body,
        out_shape=jax.ShapeDtypeStruct((2 * latent.shape[0], width), BF16),
        in_specs=[hbm] * 3,
        out_specs=vmem,
        scratch_shapes=[pltpu.SemaphoreType.DMA((4,))],
    )(down_q, down_kv, latent)


def make_heads(place, gathered_all, tokens, *arrays):
    vmem = pl.BlockSpec(memory_space=pltpu.VMEM)
    hbm = pl.BlockSpec(memory_space=pltpu.HBM)
    smem = pl.BlockSpec(memory_space=pltpu.SMEM)
    rows, width = gathered_all.shape
    down_width = QRANK + KVRANK
    return pl.pallas_call(
        make_body,
        out_shape=(
            jax.ShapeDtypeStruct((HEAD + VDIM, tokens + CTX_PAD), BF16),
            jax.ShapeDtypeStruct((HEAD, tokens), BF16),
        ),
        in_specs=[smem, hbm] + [vmem] * len(arrays),
        out_specs=(vmem, vmem),
        scratch_shapes=[
            pltpu.VMEM((rows, width - down_width), BF16),
            pltpu.VMEM((rows, down_width), BF16),
            pltpu.VMEM((tokens, 2 * (width - down_width)), BF16),
            pltpu.SemaphoreType.DMA((GROUPS + 2,)),
        ],
        cost_estimate=pl.CostEstimate(flops=6_000_000_000, bytes_accessed=0, transcendentals=0),
        compiler_params=pltpu.CompilerParams(vmem_limit_bytes=50 << 20),
    )(place, gathered_all, *arrays)


def shards(
    latent,
    context,
    cond,
    cond_context,
    mod_weight,
    norm_gain,
    down_q,
    down_kv,
    rope_weight,
    qlat_gain,
    kvlat_gain,
    up_query,
    up_key,
    up_value,
    query_gain,
    key_gain,
    context_bias,
    out_weight,
):
    seq_index = lax.axis_index(SP)
    tp_count = lax.axis_size("tp")
    own_rows = latent.shape[0]
    block_tokens = own_rows * tp_count
    row_span = mod_weight.shape[1]
    everything = lax.all_gather(pack(down_q, down_kv, latent), "tp", axis=0, tiled=True)
    out_rows = lax.all_gather(out_weight, "tp", axis=0, tiled=True)

    activated = jax.nn.silu(jnp.stack([cond, cond_context]).astype(F32)).astype(BF16)
    own_part = lax.dynamic_slice_in_dim(activated, seq_index * row_span, row_span, 1)
    partial_value = jnp.concatenate(
        [
            jnp.einsum("d,rde->re", own_part[0], mod_weight, preferred_element_type=F32),
            jnp.einsum("d,rde->re", own_part[1], mod_weight[:2], preferred_element_type=F32),
            jnp.zeros((3, mod_weight.shape[2]), F32),
        ],
        axis=0,
    )
    summed = jnp.sum(gathered(partial_value, SP).reshape((-1,) + partial_value.shape), axis=0)
    modulations = jnp.swapaxes(gathered(summed, "tp").reshape((-1,) + summed.shape), 0, 1)
    modulations = modulations.reshape(summed.shape[0], -1)

    positions = seq_index * block_tokens + jnp.arange(block_tokens, dtype=jnp.int32)
    tables = rope_tables(positions)
    latent_gain = jnp.concatenate([qlat_gain, kvlat_gain]).astype(F32)
    kv, q = make_heads(
        lax.axis_index("y").astype(jnp.int32)[None],
        everything,
        block_tokens,
        jnp.concatenate([rope_weight.T, context], axis=0),
        modulations,
        norm_gain.astype(F32)[None, :],
        latent_gain[None, :],
        jnp.concatenate(
            [
                up_query.T,
                jnp.pad(up_key.T, ((0, 0), (0, QRANK - KVRANK))),
                jnp.pad(up_value.T, ((0, 0), (0, QRANK - KVRANK))),
            ],
            axis=0,
        ),
        query_gain[:, None],
        key_gain[:, None],
        tables,
    )
    kvs = [kv] + [shifted(kv, "y", k) for k in range(1, 4)]
    qs = [shifted(q, "x", k) for k in range(1, 4)]
    bias = (context_bias + math.log(TOK_DEV / CTX_DEV)) * math.log2(math.e)

    def attend(block, chunks, *arrays, state=(), after=()):
        body = functools.partial(
            attend_body, chunks=chunks, span=256, ahead=2, block=512, resumed=len(state) > 0
        )
        shape = (VDIM + 16, block_tokens)
        flops = chunks * 50_000_000
        return kernel(body, shape, (bias,), (block, *arrays, *state), flops=flops, after=after)

    first = attend(q, 2, kvs[0], kvs[1])
    begun = attend(qs[0], 2, kvs[0], kvs[1], after=(first,))
    second = attend(qs[1], 2, kvs[0], kvs[1], after=(begun,))
    begun = attend(qs[0], 1, kvs[3], state=(begun,), after=(second,))
    theirs = [attend(qs[0], 1, kvs[2], kvs[0], kvs[1], kvs[3], state=(begun,))]
    theirs.append(
        attend(qs[1], 2, kvs[2], kvs[3], kvs[0], kvs[1], state=(second,), after=theirs)
    )
    back = [shifted(theirs[0], "x", -1), shifted(theirs[1], "x", -2)]
    theirs.append(attend(qs[2], 4, *kvs, after=theirs[1:] + back[:1]))
    back.append(shifted(theirs[2], "x", -3))
    last = attend(q, 2, kvs[2], kvs[3], kvs[0], kvs[1], after=theirs[2:] + back[1:2])
    attended = kernel(merge_body, (block_tokens, VDIM), (), (first, last, *back))

    token_rows = lax.all_to_all(attended, "tp", split_axis=0, concat_axis=1, tiled=True)
    projected = jnp.dot(token_rows, out_rows, preferred_element_type=F32)
    return (latent.astype(F32) + modulations[2] * projected).astype(BF16)


def solution(mesh):
    split = Mesh(mesh.devices.reshape(4, 4, mesh.shape["tp"]), ("y", "x", "tp"))
    placed = (
        P(SP_TP, None),
        P(SP, None),
        P(),
        P(),
        P(None, SP, "tp"),
        P(),
        P("tp", None),
        P("tp", None),
        P(),
        P(),
        P(),
        P(None, "tp"),
        P(None, "tp"),
        P(None, "tp"),
        P(),
        P(),
        P("tp"),
        P("tp", None),
    )
    return jax.shard_map(
        shards, mesh=split, in_specs=placed, out_specs=P(SP_TP, None), check_vma=False
    )
```
